256 devices in a mesh: kv: 64 (over z, y, core), tp: 4 (over x).
Axes of the slice: x: 4, y: 4, z: 8, core: 2. Of those that a mesh axis runs over, the one named last changes fastest.
Arguments:
- tokens: bfloat16 [49152, 2048], P('kv'), may hold values from -6 to 6
- w_query: bfloat16 [2048, 4096], P(None, 'tp'), may hold values from -3.1819805 to 3.1819805
- w_latent: bfloat16 [2048, 256], replicated, may hold values from -0.13258252 to 0.13258252
- latent_gain: float32 [256], replicated, may hold values from 0.1 to 1.9
- w_output: bfloat16 [4096, 2048], P('tp'), may hold values from -2 to 2
- chosen: int32 [768, 32], P('kv'), may hold values from -1 to 767, as said below
Outputs:
- attended: bfloat16 [49152, 2048], P(('kv', 'tp'))
- log_total: float32 [49152, 16], P('kv', 'tp')
The draws below stay inside these ranges and needn't reach their ends.
Inputs may be any that keep to these rules, and one draw needn't show every extreme that they name: `chosen`: row g names blocks at or before block g, no block twice; entry 0 is g itself; entries -1 name nothing and stand after the others. The 12 rows of one device together name exactly 2 distinct blocks of every earlier device's positions and none of a later device's.
All inputs are finite; a program needn't handle non-finite values.
Results may differ from the reference program's by a relative error of at most 0.01.
Values may be sent and summed in bfloat16 or wider, within the bound.
A program may use at most 192 MiB of HBM per device.

```python
import math
import jax
import jax.numpy as jnp
from jax import lax

D = 2048
HEADS = 16
R = 256
BLK = 64
NSEL = 32
CAP = 2
TOK_DEV = 768
SEQ = 49152
N_TP = 4


def latent_base(key):
    return jax.random.truncated_normal(jax.random.fold_in(key, 7), -6.0, 6.0, (D, R), jnp.float32) * D ** (-0.5)


def draw_w_latent(key, part):
    return latent_base(key).astype(jnp.bfloat16)


def draw_w_query(key, part):
    drawn = jax.random.truncated_normal(jax.random.fold_in(key, 11), -6.0, 6.0, (D, HEADS, R), jnp.float32) * D ** (-0.5)
    return drawn.reshape(D, HEADS * R).astype(jnp.bfloat16)


def draw_chosen(key, part):
    per_device = TOK_DEV // BLK
    block_count = SEQ // BLK
    devices = SEQ // TOK_DEV
    key_offer = jax.random.fold_in(key, 21)
    key_popular = jax.random.fold_in(key, 22)
    key_noise = jax.random.fold_in(key, 23)
    offer_raw = jax.random.randint(key_offer, (devices, devices, per_device), 0, 1 << 16)
    offer_score = offer_raw * per_device + jnp.arange(per_device, dtype=jnp.int32)
    offer_rank = jnp.argsort(jnp.argsort(-offer_score, axis=2), axis=2)
    offered = offer_rank < CAP
    popular = jax.random.randint(key_popular, (devices,), 0, 4)
    blocks = jnp.arange(block_count, dtype=jnp.int32)
    owner = blocks // per_device
    local_part = blocks % per_device
    dev_row = owner[:, None]
    own_col = owner[None, :]
    local_row = local_part[:, None]
    is_offered = offered[dev_row, own_col, local_part[None, :]]
    rank_here = offer_rank[dev_row, own_col, local_part[None, :]]
    earlier = blocks[None, :] <= blocks[:, None]
    other_ok = (own_col < dev_row) & is_offered
    allowed = (own_col == dev_row) & earlier | other_ok
    forced = other_ok & ((own_col * CAP + rank_here) % per_device == local_row)
    hot = (own_col == 0) | (own_col == dev_row - 1) | (own_col == dev_row - devices // 2)
    bias = jnp.where(blocks[None, :] == blocks[:, None], 40, jnp.where(forced, 30, jnp.where(own_col == dev_row, 8, jnp.where(hot, 20, 2 * popular[own_col]))))
    noise = jax.random.randint(key_noise, (block_count, block_count), 0, 4096)
    score = (bias * 4096 + noise) * block_count + blocks[None, :]
    score = jnp.where(allowed, score, -1 - blocks[None, :])
    values, picked = lax.top_k(score, NSEL)
    return jnp.where(values >= 0, picked, -1).astype(jnp.int32)


def steps_of(stream_key, shape, split, smallest, high):
    def one(dim, blocks):
        steps = jax.random.uniform(jax.random.fold_in(jax.random.fold_in(stream_key, 6), dim), (blocks,), jnp.float32, smallest / len(split), high / len(split))
        return jnp.repeat(jnp.exp(steps), shape[dim] // blocks).reshape((-1,) + (1,) * (len(shape) - dim - 1))

    gain = one(*split[0])
    for cut in split[1:]:
        gain = gain * one(*cut)
    return gain


def normal_values(key, shape, scale, most, shards=(), kind=jnp.bfloat16):
    values = scale * jax.random.normal(key, shape, jnp.float32)
    if shards:
        values = values * steps_of(key, shape, shards, -0.22, 0.18)
    return jnp.clip(values, -most, most).astype(kind)


def setup_inputs(seed: int = 0) -> dict:
    key_of = jax.random.split(jax.random.key(seed), 7)
    tokens = normal_values(key_of[0], (SEQ, D), 1.0, 6.0, ((0, 64),))
    w_query = draw_w_query(jax.random.fold_in(key_of[6], 71), 0)
    w_latent = draw_w_latent(jax.random.fold_in(key_of[6], 71), 0)
    latent_gain = jnp.clip(1.0 + 0.18 * jax.random.normal(key_of[3], (R,), jnp.float32), 0.1, 1.9)
    w_output = normal_values(key_of[4], (HEADS * R, D), 8 ** -0.5, 2.0, ((0, 4),))
    chosen = draw_chosen(jax.random.fold_in(key_of[6], 71), 0)
    return {"tokens": tokens, "w_query": w_query, "w_latent": w_latent, "latent_gain": latent_gain, "w_output": w_output, "chosen": chosen}


epsilon = 1e-06

def latents_of(tokens, w_latent, latent_gain):
    projected = jnp.dot(tokens, w_latent, preferred_element_type=jnp.float32)
    inv_rms = lax.rsqrt(lax.optimization_barrier(jnp.mean(projected * projected, axis=-1, keepdims=True)) + epsilon)
    return (projected * inv_rms * latent_gain).astype(jnp.bfloat16)

def attend(query_part, key_rows, picked, query_blocks, blk_len, score_scale):
    group_size, picks_each = picked.shape
    offsets = jnp.arange(blk_len, dtype=jnp.int32)
    key_pos = (picked[:, :, None] * blk_len + offsets[None, None, :]).reshape(group_size, picks_each * blk_len)
    usable = jnp.repeat(picked >= 0, blk_len, axis=1)
    query_pos = query_blocks[:, None] * blk_len + offsets[None, :]
    allowed = usable[:, None, :] & (key_pos[:, None, :] <= query_pos[:, :, None])
    scores = jnp.einsum('gqhr,gkr->ghqk', query_part.astype(jnp.float32), key_rows.astype(jnp.float32)) * score_scale
    scores = jnp.where(allowed[:, None, :, :], scores, -jnp.inf)
    peak_score = lax.optimization_barrier(jnp.max(scores, axis=3, keepdims=True))
    raised = jnp.exp(scores - peak_score)
    total_mass = lax.optimization_barrier(jnp.sum(raised, axis=3))
    weights = raised.astype(jnp.bfloat16)
    summed = jnp.einsum('ghqk,gkr->gqhr', weights.astype(jnp.float32), key_rows.astype(jnp.float32))
    mass_t = jnp.transpose(total_mass, (0, 2, 1))
    heads_out = (summed / mass_t[..., None]).astype(jnp.bfloat16)
    log_part = jnp.transpose(peak_score[..., 0], (0, 2, 1)) + jnp.log(mass_t)
    return (heads_out, log_part)

def reference(tokens, w_query, w_latent, latent_gain, w_output, chosen):
    seq_len, width = tokens.shape
    lat_rank = w_latent.shape[1]
    head_count = w_query.shape[1] // lat_rank
    block_count, picks_each = chosen.shape
    blk_len = seq_len // block_count
    latent = latents_of(tokens, w_latent, latent_gain)
    queries = jnp.dot(tokens, w_query, preferred_element_type=jnp.float32).astype(jnp.bfloat16)
    queries = queries.reshape(block_count, blk_len, head_count, lat_rank)
    key_table = latent.reshape(block_count, blk_len, lat_rank)
    group_size = math.gcd(block_count, 8)
    score_scale = lat_rank ** (-0.5)

    def one_group(offset):
        picked = lax.dynamic_slice_in_dim(chosen, offset, group_size, 0)
        query_part = lax.dynamic_slice_in_dim(queries, offset, group_size, 0)
        key_rows = jnp.take(key_table, jnp.maximum(picked, 0), axis=0).reshape(group_size, picks_each * blk_len, lat_rank)
        query_blocks = offset + jnp.arange(group_size, dtype=jnp.int32)
        return attend(query_part, key_rows, picked, query_blocks, blk_len, score_scale)
    group_starts = jnp.arange(0, block_count, group_size, dtype=jnp.int32)
    heads_out, log_total = lax.map(one_group, group_starts)
    heads_flat = heads_out.reshape(seq_len, head_count * lat_rank)
    log_total = log_total.reshape(seq_len, head_count)
    group_cols = head_count // N_TP * lat_rank
    attended = jnp.zeros((seq_len, width), jnp.float32)
    for group_index in range(N_TP):
        low = group_index * group_cols
        partial_value = jnp.dot(heads_flat[:, low:low + group_cols], w_output[low:low + group_cols], preferred_element_type=jnp.float32)
        attended = attended + lax.optimization_barrier(partial_value.astype(jnp.bfloat16)).astype(jnp.float32)
    return (attended.astype(jnp.bfloat16), log_total)
```

```python
import functools

import jax
import jax.numpy as jnp
from jax import lax
from jax.experimental import pallas as pl
from jax.experimental.pallas import tpu as pltpu
from jax.sharding import PartitionSpec as P

EPS = 1e-06
KV = 64
TP = 4
GRP = 8
BLK = 64
HALF = 32
R = 256
PER = 12
NSEL = 32
OWN = TP * KV
SLOTS = OWN + 2 * PER
ROWS = PER * BLK
HEADS = 4


def remote(src, dst, send_sem, recv_sem, kv, tp):
    return pltpu.make_async_remote_copy(
        src_ref=src,
        dst_ref=dst,
        send_sem=send_sem,
        recv_sem=recv_sem,
        device_id={"kv": kv, "tp": tp},
        device_id_type=pl.DeviceIdType.MESH,
    )


def fetch_kernel(
    tok_hbm, wl_ref, gain_ref, wq_hbm, req_ref,
    table_ref, q_ref,
    tok_v, wq_v, own_v, sendbuf, reqin, req_smem,
    tok_sem, wq_sem, loc_sem, rs_sem, rr_sem, ds_sem, dr_sem, xs_sem, xl_sem, xr_sem, xd_sem,
):
    me = lax.axis_index("kv")
    x = lax.axis_index("tp")
    mz = me // GRP
    myc = me % GRP
    left = (x + TP - 1) % TP
    right = (x + 1) % TP

    reqin[...] = jnp.zeros_like(reqin)
    barrier = pltpu.get_barrier_semaphore()

    @pl.loop(0, KV)
    def _(i):
        @pl.when(i != me)
        def _():
            pl.semaphore_signal(
                barrier, inc=1, device_id={"kv": i, "tp": x}, device_id_type=pl.DeviceIdType.MESH
            )

    for nb in (left, right):
        pl.semaphore_signal(
            barrier, inc=1, device_id={"kv": me, "tp": nb}, device_id_type=pl.DeviceIdType.MESH
        )

    def tok_copy(i):
        rows = pl.ds(i * 128, 128)
        return pltpu.make_async_copy(tok_hbm.at[rows], tok_v.at[rows], tok_sem.at[i])

    def wq_copy(h):
        cols = pl.ds(h * R, R)
        return pltpu.make_async_copy(wq_hbm.at[:, cols], wq_v.at[:, cols], wq_sem.at[h])

    for i in range(6):
        tok_copy(i).start()
    for h in range(HEADS):
        wq_copy(h).start()
    for i in range(6):
        tok_copy(i).wait()
        p = jnp.dot(tok_v[i * 128 : (i + 1) * 128, :], wl_ref[...], preferred_element_type=jnp.float32)
        inv = lax.rsqrt(jnp.mean(p * p, axis=-1, keepdims=True) + EPS)
        lat = (p * inv * gain_ref[...]).astype(jnp.bfloat16)
        own_v[4 * i : 4 * i + 4] = lat.reshape(4, HALF, R)
        table_ref[OWN + 4 * i : OWN + 4 * i + 4] = lat.reshape(4, HALF, R)

    pl.semaphore_wait(barrier, KV - 1 + 2)

    def req_copy(i):
        return remote(req_ref.at[i], reqin.at[me], rs_sem.at[i], rr_sem.at[me], i, x)

    @pl.loop(0, me)
    def _(i):
        req_copy(i).start()

    @pl.loop(me + 1, KV)
    def _(i):
        remote(req_ref.at[i], reqin.at[i], rs_sem.at[i], rr_sem.at[i], i, x).wait_recv()

    to_smem = pltpu.make_async_copy(reqin, req_smem, loc_sem)
    to_smem.start()
    to_smem.wait()

    def data_copy(d):
        return remote(
            sendbuf.at[d],
            table_ref.at[x * KV + me],
            ds_sem.at[d],
            dr_sem.at[jnp.where(d // GRP == mz, GRP + myc, mz)],
            d,
            x,
        )

    @pl.loop(0, GRP - mz)
    def _(s):
        base = (GRP - 1 - s) * GRP

        @pl.loop(0, GRP)
        def _(k):
            d = base + (myc + k) % GRP

            @pl.when(d > me)
            def _():
                sendbuf[d] = own_v[req_smem[d, 0, 0]]

        @pl.loop(0, GRP)
        def _(k):
            d = base + (myc + k) % GRP

            @pl.when(d > me)
            def _():
                data_copy(d).start()

    for h in range(HEADS):
        wq_copy(h).wait()
        q = jnp.dot(tok_v[...], wq_v[:, h * R : (h + 1) * R], preferred_element_type=jnp.float32)
        q_ref[:, h * R : (h + 1) * R] = (q.astype(jnp.bfloat16).astype(jnp.float32) * (R ** -0.5)).astype(jnp.bfloat16)

    def region(quarter, z):
        return table_ref.at[pl.ds(quarter * KV + z * GRP, GRP)]

    def to_right(z):
        return remote(region(x, z), region(x, z), xs_sem.at[0, z], xl_sem.at[z], me, right)

    def to_left(z):
        return remote(region(x, z), region(x, z), xs_sem.at[1, z], xr_sem.at[z], me, left)

    def pass_right(z):
        return remote(region(left, z), region(left, z), xs_sem.at[2, z], xd_sem.at[z], me, right)

    def pass_left(z):
        return remote(region(right, z), region(right, z), xs_sem.at[2, z], xd_sem.at[z], me, left)

    def group_done(z):
        pltpu.make_async_copy(region(x, z), region(x, z), dr_sem.at[z]).wait()

    for dist in (1, 7, 2, 6, 3, 5, 4):
        @pl.when(mz >= dist)
        def _(dist=dist):
            z = mz - dist
            group_done(z)
            to_right(z).start()
            to_left(z).start()

    @pl.when(myc > 0)
    def _():
        @pl.loop(0, myc)
        def _(k):
            one = table_ref.at[x * KV + mz * GRP + k]
            pltpu.make_async_copy(one, one, dr_sem.at[GRP + k]).wait()

        to_right(mz).start()
        to_left(mz).start()

    for dist in (1, 7, 2, 6, 3, 5, 4, 0):
        z = mz - dist

        @pl.when((z >= 0) & ((dist != 0) | (myc > 0)))
        def _(z=z):
            to_right(z).wait_recv()
            to_left(z).wait_recv()

            @pl.when(z % 2 == 0)
            def _():
                pass_right(z).start()

            @pl.when(z % 2 == 1)
            def _():
                pass_left(z).start()

    for dist in (1, 7, 2, 6, 3, 5, 4, 0):
        z = mz - dist

        @pl.when((z >= 0) & ((dist != 0) | (myc > 0)))
        def _(z=z):
            pass_right(z).wait_recv()
            to_right(z).wait_send()
            to_left(z).wait_send()
            pass_right(z).wait_send()

    @pl.loop(0, me)
    def _(i):
        req_copy(i).wait_send()

    @pl.loop(me + 1, KV)
    def _(d):
        data_copy(d).wait_send()


def fetch(tokens, w_latent, gain, w_query, req):
    vmem = pl.BlockSpec(memory_space=pltpu.VMEM)
    anyspace = pl.BlockSpec(memory_space=pl.ANY)
    dma = pltpu.SemaphoreType.DMA
    return pl.pallas_call(
        fetch_kernel,
        out_shape=(
            jax.ShapeDtypeStruct((SLOTS, HALF, R), jnp.bfloat16),
            jax.ShapeDtypeStruct((ROWS, HEADS * R), jnp.bfloat16),
        ),
        in_specs=[anyspace, vmem, vmem, anyspace, vmem],
        out_specs=(vmem, vmem),
        scratch_shapes=[
            pltpu.VMEM(tokens.shape, jnp.bfloat16),
            pltpu.VMEM(w_query.shape, jnp.bfloat16),
            pltpu.VMEM((2 * PER, HALF, R), jnp.bfloat16),
            pltpu.VMEM((KV, HALF, R), jnp.bfloat16),
            pltpu.VMEM((KV, 1, 128), jnp.int32),
            pltpu.SMEM((KV, 1, 128), jnp.int32),
            dma((6,)),
            dma((HEADS,)),
            dma,
            dma((KV,)),
            dma((KV,)),
            dma((KV,)),
            dma((2 * GRP,)),
            dma((3, GRP)),
            dma((GRP,)),
            dma((GRP,)),
            dma((GRP,)),
        ],
        compiler_params=pltpu.CompilerParams(
            collective_id=0, has_side_effects=True, vmem_limit_bytes=48 * 1024 * 1024
        ),
        name="fetch",
    )(tokens, w_latent, gain, w_query, req)


def attend_kernel(idx_ref, cnt_ref, q_ref, table_ref, out_ref, log_ref, kbuf, s_scr, p_scr):
    g = pl.program_id(0)
    base = g * (2 * NSEL)
    for j in range(2 * NSEL):
        kbuf[j * HALF : (j + 1) * HALF, :] = table_ref[idx_ref[base + j]]
    q = jnp.concatenate([q_ref[:, h * R : (h + 1) * R] for h in range(HEADS)], axis=0)
    live = cnt_ref[g] * BLK
    rows = HEADS * BLK
    step = 512
    top = None
    for c in range(NSEL * BLK // step):
        s = lax.dot_general(
            q, kbuf[c * step : (c + 1) * step, :], (((1,), (1,)), ((), ())),
            preferred_element_type=jnp.float32,
        )
        col = lax.broadcasted_iota(jnp.int32, (rows, step), 1)
        ok = col + c * step < live
        if c == 0:
            t = lax.broadcasted_iota(jnp.int32, (rows, step), 0) % BLK
            ok = ok & ((col >= BLK) | (col <= t))
        s = jnp.where(ok, s, -jnp.inf)
        s_scr[:, c * step : (c + 1) * step] = s
        for k in range(step // 128):
            part = s[:, k * 128 : (k + 1) * 128]
            top = part if top is None else jnp.maximum(top, part)
    peak = jnp.max(top, axis=1, keepdims=True)
    total = None
    for c in range(NSEL * BLK // step):
        e = jnp.exp(s_scr[:, c * step : (c + 1) * step] - peak)
        p_scr[:, c * step : (c + 1) * step] = e.astype(jnp.bfloat16)
        for k in range(step // 128):
            part = e[:, k * 128 : (k + 1) * 128]
            total = part if total is None else total + part
    mass = jnp.sum(total, axis=1, keepdims=True)
    o = jnp.dot(p_scr[...], kbuf[...], preferred_element_type=jnp.float32) / mass
    logs = peak + jnp.log(mass)
    for h in range(HEADS):
        out_ref[:, h * R : (h + 1) * R] = o[h * BLK : (h + 1) * BLK].astype(jnp.bfloat16)
        log_ref[:, h : h + 1] = logs[h * BLK : (h + 1) * BLK]


def attention(idx, cnt, q, table):
    return pl.pallas_call(
        attend_kernel,
        grid_spec=pltpu.PrefetchScalarGridSpec(
            num_scalar_prefetch=2,
            grid=(PER,),
            in_specs=[
                pl.BlockSpec((BLK, HEADS * R), lambda g, *_: (g, 0)),
                pl.BlockSpec((SLOTS, HALF, R), lambda g, *_: (0, 0, 0)),
            ],
            out_specs=[
                pl.BlockSpec((BLK, HEADS * R), lambda g, *_: (g, 0)),
                pl.BlockSpec((BLK, HEADS), lambda g, *_: (g, 0)),
            ],
            scratch_shapes=[
                pltpu.VMEM((NSEL * BLK, R), jnp.bfloat16),
                pltpu.VMEM((HEADS * BLK, NSEL * BLK), jnp.float32),
                pltpu.VMEM((HEADS * BLK, NSEL * BLK), jnp.bfloat16),
            ],
        ),
        out_shape=(
            jax.ShapeDtypeStruct((ROWS, HEADS * R), jnp.bfloat16),
            jax.ShapeDtypeStruct((ROWS, HEADS), jnp.float32),
        ),
        compiler_params=pltpu.CompilerParams(vmem_limit_bytes=48 * 1024 * 1024),
        name="attend",
    )(idx, cnt, q, table)


def plan(chosen):
    me = lax.axis_index("kv")
    x = lax.axis_index("tp")
    flat = chosen.reshape(PER * NSEL)
    valid = flat >= 0
    owner = jnp.where(valid, flat // PER, -1)
    owners = jnp.arange(KV, dtype=jnp.int32)
    hit = owner[None, :] == owners[:, None]
    lo = jnp.min(jnp.where(hit, flat[None, :], KV * PER), axis=1)
    hi = jnp.max(jnp.where(hit, flat[None, :], -1), axis=1)
    pick = jnp.where(x < 2, lo, hi) - owners * PER
    req = jnp.clip(pick, 0, PER - 1) * 2 + x % 2
    req = jnp.broadcast_to(req[:, None, None], (KV, 1, 128))
    later = jnp.any(hit & (flat[None, :] > lo[:, None]), axis=0)
    own0 = OWN + 2 * (flat - me * PER)
    far0 = 2 * KV * later.astype(jnp.int32) + owner
    mine = owner == me
    first = jnp.where(valid, jnp.where(mine, own0, far0), OWN)
    second = jnp.where(valid, first + jnp.where(mine, 1, KV), OWN)
    idx = jnp.stack([first, second], axis=1).reshape(-1)
    cnt = jnp.sum((chosen >= 0).astype(jnp.int32), axis=1)
    return req, idx, cnt


def local(tokens, w_query, w_latent, latent_gain, w_output, chosen):
    req, idx, cnt = plan(chosen)
    table, q = fetch(tokens, w_latent, latent_gain.reshape(1, R), w_query, req)
    heads, logs = attention(idx, cnt, q, table)
    partial = jnp.dot(heads, w_output, preferred_element_type=jnp.float32).astype(jnp.bfloat16)
    parts = lax.all_to_all(partial.reshape(TP, ROWS // TP, -1), "tp", 0, 0, tiled=True)
    attended = jnp.sum(parts.astype(jnp.float32), axis=0).astype(jnp.bfloat16)
    return attended, logs


def solution(mesh):
    placed = (P("kv", None), P(None, "tp"), P(), P(), P("tp", None), P("kv", None))
    return jax.shard_map(
        local,
        mesh=mesh,
        in_specs=placed,
        out_specs=(P(("kv", "tp"), None), P("kv", "tp")),
        check_vma=False,
    )
```

```python
import functools

import jax
import jax.numpy as jnp
from jax import lax
from jax.experimental import pallas as pl
from jax.experimental.pallas import tpu as pltpu
from jax.sharding import PartitionSpec as P

EPS = 1e-06
KV = 64
TP = 4
GRP = 8
BLK = 64
HALF = 32
R = 256
PER = 12
NSEL = 32
OWN = TP * KV
SLOTS = OWN + 2 * PER
ROWS = PER * BLK
HEADS = 4


def remote(src, dst, send_sem, recv_sem, kv, tp):
    return pltpu.make_async_remote_copy(
        src_ref=src,
        dst_ref=dst,
        send_sem=send_sem,
        recv_sem=recv_sem,
        device_id={"kv": kv, "tp": tp},
        device_id_type=pl.DeviceIdType.MESH,
    )


def fetch_kernel(
    tok_hbm, wl_ref, gain_ref, wq_hbm, req_ref,
    table_ref, q_ref,
    tok_v, wq_v, own_v, sendbuf, reqin, req_smem,
    tok_sem, wq_sem, loc_sem, rs_sem, rr_sem, ds_sem, dr_sem, xs_sem, xl_sem, xr_sem, xd_sem,
):
    me = lax.axis_index("kv")
    x = lax.axis_index("tp")
    mz = me // GRP
    myc = me % GRP
    left = (x + TP - 1) % TP
    right = (x + 1) % TP

    reqin[...] = jnp.zeros_like(reqin)
    barrier = pltpu.get_barrier_semaphore()

    @pl.loop(0, KV)
    def _(i):
        @pl.when(i != me)
        def _():
            pl.semaphore_signal(
                barrier, inc=1, device_id={"kv": i, "tp": x}, device_id_type=pl.DeviceIdType.MESH
            )

    for nb in (left, right):
        pl.semaphore_signal(
            barrier, inc=1, device_id={"kv": me, "tp": nb}, device_id_type=pl.DeviceIdType.MESH
        )

    def tok_copy(i):
        rows = pl.ds(i * 128, 128)
        return pltpu.make_async_copy(tok_hbm.at[rows], tok_v.at[rows], tok_sem.at[i])

    def wq_copy(h):
        cols = pl.ds(h * R, R)
        return pltpu.make_async_copy(wq_hbm.at[:, cols], wq_v.at[:, cols], wq_sem.at[h])

    for i in range(6):
        tok_copy(i).start()
    for h in range(HEADS):
        wq_copy(h).start()
    for i in range(6):
        tok_copy(i).wait()
        p = jnp.dot(tok_v[i * 128 : (i + 1) * 128, :], wl_ref[...], preferred_element_type=jnp.float32)
        inv = lax.rsqrt(jnp.mean(p * p, axis=-1, keepdims=True) + EPS)
        lat = (p * inv * gain_ref[...]).astype(jnp.bfloat16)
        own_v[4 * i : 4 * i + 4] = lat.reshape(4, HALF, R)
        table_ref[OWN + 4 * i : OWN + 4 * i + 4] = lat.reshape(4, HALF, R)

    pl.semaphore_wait(barrier, KV - 1 + 2)

    def req_copy(i):
        return remote(req_ref.at[i], reqin.at[me], rs_sem.at[i], rr_sem.at[me], i, x)

    @pl.loop(0, me)
    def _(i):
        req_copy(i).start()

    @pl.loop(me + 1, KV)
    def _(i):
        remote(req_ref.at[i], reqin.at[i], rs_sem.at[i], rr_sem.at[i], i, x).wait_recv()

    to_smem = pltpu.make_async_copy(reqin, req_smem, loc_sem)
    to_smem.start()
    to_smem.wait()

    def data_copy(d):
        return remote(
            sendbuf.at[d],
            table_ref.at[x * KV + me],
            ds_sem.at[d],
            dr_sem.at[jnp.where(d // GRP == mz, GRP + myc, mz)],
            d,
            x,
        )

    @pl.loop(0, GRP - mz)
    def _(s):
        base = (GRP - 1 - s) * GRP

        @pl.loop(0, GRP)
        def _(k):
            d = base + (myc + k) % GRP

            @pl.when(d > me)
            def _():
                sendbuf[d] = own_v[req_smem[d, 0, 0]]

        @pl.loop(0, GRP)
        def _(k):
            d = base + (myc + k) % GRP

            @pl.when(d > me)
            def _():
                data_copy(d).start()

    for h in range(HEADS):
        wq_copy(h).wait()
        q = jnp.dot(tok_v[...], wq_v[:, h * R : (h + 1) * R], preferred_element_type=jnp.float32)
        q_ref[:, h * R : (h + 1) * R] = (q.astype(jnp.bfloat16).astype(jnp.float32) * (R ** -0.5)).astype(jnp.bfloat16)

    def region(quarter, z):
        return table_ref.at[pl.ds(quarter * KV + z * GRP, GRP)]

    def to_right(z):
        return remote(region(x, z), region(x, z), xs_sem.at[0, z], xl_sem.at[z], me, right)

    def to_left(z):
        return remote(region(x, z), region(x, z), xs_sem.at[1, z], xr_sem.at[z], me, left)

    def pass_right(z):
        return remote(region(left, z), region(left, z), xs_sem.at[2, z], xd_sem.at[z], me, right)

    def pass_left(z):
        return remote(region(right, z), region(right, z), xs_sem.at[2, z], xd_sem.at[z], me, left)

    def group_done(z):
        pltpu.make_async_copy(region(x, z), region(x, z), dr_sem.at[z]).wait()

    for dist in (1, 7, 2, 6, 3, 5, 4):
        @pl.when(mz >= dist)
        def _(dist=dist):
            z = mz - dist
            group_done(z)
            to_right(z).start()
            to_left(z).start()

    @pl.when(myc > 0)
    def _():
        @pl.loop(0, myc)
        def _(k):
            one = table_ref.at[x * KV + mz * GRP + k]
            pltpu.make_async_copy(one, one, dr_sem.at[GRP + k]).wait()

        to_right(mz).start()
        to_left(mz).start()

    for dist in (1, 7, 2, 6, 3, 5, 4, 0):
        z = mz - dist

        @pl.when((z >= 0) & ((dist != 0) | (myc > 0)))
        def _(z=z):
            to_right(z).wait_recv()
            to_left(z).wait_recv()

            @pl.when(z % 2 == 0)
            def _():
                pass_right(z).start()

            @pl.when(z % 2 == 1)
            def _():
                pass_left(z).start()

    for dist in (1, 7, 2, 6, 3, 5, 4, 0):
        z = mz - dist

        @pl.when((z >= 0) & ((dist != 0) | (myc > 0)))
        def _(z=z):
            pass_right(z).wait_recv()
            to_right(z).wait_send()
            to_left(z).wait_send()
            pass_right(z).wait_send()

    @pl.loop(0, me)
    def _(i):
        req_copy(i).wait_send()

    @pl.loop(me + 1, KV)
    def _(d):
        data_copy(d).wait_send()


def fetch(tokens, w_latent, gain, w_query, req):
    vmem = pl.BlockSpec(memory_space=pltpu.VMEM)
    anyspace = pl.BlockSpec(memory_space=pltpu.HBM)
    dma = pltpu.SemaphoreType.DMA
    return pl.pallas_call(
        fetch_kernel,
        out_shape=(
            jax.ShapeDtypeStruct((SLOTS, HALF, R), jnp.bfloat16),
            jax.ShapeDtypeStruct((ROWS, HEADS * R), jnp.bfloat16),
        ),
        in_specs=[anyspace, vmem, vmem, anyspace, vmem],
        out_specs=(vmem, vmem),
        scratch_shapes=[
            pltpu.VMEM(tokens.shape, jnp.bfloat16),
            pltpu.VMEM(w_query.shape, jnp.bfloat16),
            pltpu.VMEM((2 * PER, HALF, R), jnp.bfloat16),
            pltpu.VMEM((KV, HALF, R), jnp.bfloat16),
            pltpu.VMEM((KV, 1, 128), jnp.int32),
            pltpu.SMEM((KV, 1, 128), jnp.int32),
            dma((6,)),
            dma((HEADS,)),
            dma,
            dma((KV,)),
            dma((KV,)),
            dma((KV,)),
            dma((2 * GRP,)),
            dma((3, GRP)),
            dma((GRP,)),
            dma((GRP,)),
            dma((GRP,)),
        ],
        compiler_params=pltpu.CompilerParams(
            collective_id=0, has_side_effects=True, vmem_limit_bytes=48 * 1024 * 1024
        ),
        name="fetch",
    )(tokens, w_latent, gain, w_query, req)


def finish_kernel(
    idx_ref, cnt_ref, q_ref, table_ref, wo_ref,
    out_ref, log_ref,
    kbuf, s_scr, m_scr, heads, stage, got,
    snd_sem, got_sem,
):
    me = lax.axis_index("kv")
    x = lax.axis_index("tp")
    left = (x + TP - 1) % TP
    right = (x + 1) % TP
    barrier = pltpu.get_barrier_semaphore()
    for nb in (left, right):
        pl.semaphore_signal(
            barrier, inc=1, device_id={"kv": me, "tp": nb}, device_id_type=pl.DeviceIdType.MESH
        )

    def dest(it):
        off = jnp.where(it == 0, 2, jnp.where(it == 1, 1, jnp.where(it == 2, 3, 0)))
        return (x + off) % TP

    rows = HEADS * BLK
    keys = NSEL * BLK
    step = 512

    def scores(b, slot):
        for j in range(2 * NSEL):
            kbuf[slot, j * HALF : (j + 1) * HALF, :] = table_ref[idx_ref[b * (2 * NSEL) + j]]
        here = pl.ds(pl.multiple_of(b * BLK, BLK), BLK)
        q = jnp.concatenate([q_ref[here, h * R : (h + 1) * R] for h in range(HEADS)], axis=0)
        live = cnt_ref[b] * BLK
        top = None
        for c in range(keys // step):
            s = lax.dot_general(
                q, kbuf[slot, c * step : (c + 1) * step, :], (((1,), (1,)), ((), ())),
                preferred_element_type=jnp.float32,
            )
            col = lax.broadcasted_iota(jnp.int32, (rows, step), 1)
            ok = col + c * step < live
            if c == 0:
                t = lax.broadcasted_iota(jnp.int32, (rows, step), 0) % BLK
                ok = ok & ((col >= BLK) | (col <= t))
            s = jnp.where(ok, s, -jnp.inf)
            s_scr[slot, :, c * step : (c + 1) * step] = s
            for k in range(step // 128):
                part = s[:, k * 128 : (k + 1) * 128]
                top = part if top is None else jnp.maximum(top, part)
        m_scr[slot] = top

    def values(b, slot, j):
        peak = jnp.max(m_scr[slot], axis=1, keepdims=True)
        total = None
        o = None
        for c in range(keys // step):
            e = jnp.exp(s_scr[slot, :, c * step : (c + 1) * step] - peak)
            for k in range(step // 128):
                part = e[:, k * 128 : (k + 1) * 128]
                total = part if total is None else total + part
            oc = jnp.dot(
                e.astype(jnp.bfloat16), kbuf[slot, c * step : (c + 1) * step, :],
                preferred_element_type=jnp.float32,
            )
            o = oc if o is None else o + oc
        mass = jnp.sum(total, axis=1, keepdims=True)
        o = o / mass
        logs = peak + jnp.log(mass)
        here = pl.ds(pl.multiple_of(b * BLK, BLK), BLK)
        for h in range(HEADS):
            heads[j * BLK : (j + 1) * BLK, h * R : (h + 1) * R] = o[h * BLK : (h + 1) * BLK].astype(jnp.bfloat16)
            log_ref[here, h : h + 1] = logs[h * BLK : (h + 1) * BLK]

    def move(k):
        src, slot, nb = (
            (stage.at[0, 0], 0, right),
            (stage.at[0, 1], 1, left),
            (stage.at[1, 1], 2, right),
            (stage.at[2, 0], 3, left),
            (stage.at[1, 0], 4, right),
            (stage.at[2, 1], 5, left),
        )[k]
        return remote(src, got.at[slot], snd_sem.at[k], got_sem.at[slot], me, nb)

    scores(3 * dest(0), 0)

    @pl.loop(0, TP)
    def _(it):
        b0 = 3 * dest(it)
        nxt = jnp.where(it == TP - 1, b0, 3 * dest(it + 1))
        for j in range(3):
            scores(b0 + j + 1 if j < 2 else nxt, (j + 1) % 3)
            values(b0 + j, j, j)
        for n in range(8):
            part = jnp.dot(heads[...], wo_ref[:, n * 256 : (n + 1) * 256], preferred_element_type=jnp.float32)
            stage[it, n // 4, :, (n % 4) * 256 : (n % 4 + 1) * 256] = part.astype(jnp.bfloat16)

        @pl.when(it == 0)
        def _():
            pl.semaphore_wait(barrier, 2)
            move(0).start()
            move(1).start()

        @pl.when(it == 1)
        def _():
            move(2).start()

        @pl.when(it == 2)
        def _():
            move(3).start()

    f32 = jnp.float32
    move(0).wait_recv()
    stage[1, 0] = (stage[1, 0].astype(f32) + got[0].astype(f32)).astype(jnp.bfloat16)
    move(4).start()
    move(1).wait_recv()
    stage[2, 1] = (stage[2, 1].astype(f32) + got[1].astype(f32)).astype(jnp.bfloat16)
    move(5).start()
    half = 1024
    for k, h in ((0, 0), (1, 1)):
        move(3 - k).wait_recv()
        move(4 + k).wait_recv()
        lo = 3 if h == 0 else 2
        hi = 4 if h == 0 else 5
        total = stage[3, h].astype(f32) + got[lo].astype(f32) + got[hi].astype(f32)
        out_ref[:, h * half : (h + 1) * half] = total.astype(jnp.bfloat16)
    for k in range(6):
        move(k).wait_send()


def finish(idx, cnt, q, table, w_output):
    vmem = pl.BlockSpec(memory_space=pltpu.VMEM)
    smem = pl.BlockSpec(memory_space=pltpu.SMEM)
    part = ROWS // TP
    return pl.pallas_call(
        finish_kernel,
        out_shape=(
            jax.ShapeDtypeStruct((part, 2048), jnp.bfloat16),
            jax.ShapeDtypeStruct((ROWS, HEADS), jnp.float32),
        ),
        in_specs=[smem, smem, vmem, vmem, vmem],
        out_specs=(vmem, vmem),
        scratch_shapes=[
            pltpu.VMEM((3, NSEL * BLK, R), jnp.bfloat16),
            pltpu.VMEM((3, HEADS * BLK, NSEL * BLK), jnp.float32),
            pltpu.VMEM((3, HEADS * BLK, 128), jnp.float32),
            pltpu.VMEM((part, HEADS * R), jnp.bfloat16),
            pltpu.VMEM((TP, 2, part, 1024), jnp.bfloat16),
            pltpu.VMEM((6, part, 1024), jnp.bfloat16),
            pltpu.SemaphoreType.DMA((6,)),
            pltpu.SemaphoreType.DMA((6,)),
        ],
        compiler_params=pltpu.CompilerParams(
            collective_id=1, has_side_effects=True, vmem_limit_bytes=48 * 1024 * 1024
        ),
        name="finish",
    )(idx, cnt, q, table, w_output)


def plan(chosen):
    me = lax.axis_index("kv")
    x = lax.axis_index("tp")
    flat = chosen.reshape(PER * NSEL)
    valid = flat >= 0
    owner = jnp.where(valid, flat // PER, -1)
    owners = jnp.arange(KV, dtype=jnp.int32)
    hit = owner[None, :] == owners[:, None]
    lo = jnp.min(jnp.where(hit, flat[None, :], KV * PER), axis=1)
    hi = jnp.max(jnp.where(hit, flat[None, :], -1), axis=1)
    pick = jnp.where(x < 2, lo, hi) - owners * PER
    req = jnp.clip(pick, 0, PER - 1) * 2 + x % 2
    req = jnp.broadcast_to(req[:, None, None], (KV, 1, 128))
    later = jnp.any(hit & (flat[None, :] > lo[:, None]), axis=0)
    own0 = OWN + 2 * (flat - me * PER)
    far0 = 2 * KV * later.astype(jnp.int32) + owner
    mine = owner == me
    first = jnp.where(valid, jnp.where(mine, own0, far0), OWN)
    second = jnp.where(valid, first + jnp.where(mine, 1, KV), OWN)
    idx = jnp.stack([first, second], axis=1).reshape(-1)
    cnt = jnp.sum((chosen >= 0).astype(jnp.int32), axis=1)
    return req, idx, cnt


def local(tokens, w_query, w_latent, latent_gain, w_output, chosen):
    req, idx, cnt = plan(chosen)
    table, q = fetch(tokens, w_latent, latent_gain.reshape(1, R), w_query, req)
    attended, logs = finish(idx, cnt, q, table, w_output)
    return attended, logs


def solution(mesh):
    placed = (P("kv", None), P(None, "tp"), P(), P(), P("tp", None), P("kv", None))
    return jax.shard_map(
        local,
        mesh=mesh,
        in_specs=placed,
        out_specs=(P(("kv", "tp"), None), P("kv", "tp")),
        check_vma=False,
    )
```

```python
import functools

import jax
import jax.numpy as jnp
from jax import lax
from jax.experimental import pallas as pl
from jax.experimental.pallas import tpu as pltpu
from jax.sharding import PartitionSpec as P

EPS = 1e-06
KV = 64
TP = 4
GRP = 8
BLK = 64
HALF = 32
R = 256
PER = 12
NSEL = 32
OWN = TP * KV
SLOTS = OWN + 2 * PER
ROWS = PER * BLK
HEADS = 4


def remote(src, dst, send_sem, recv_sem, kv, tp):
    return pltpu.make_async_remote_copy(
        src_ref=src,
        dst_ref=dst,
        send_sem=send_sem,
        recv_sem=recv_sem,
        device_id={"kv": kv, "tp": tp},
        device_id_type=pl.DeviceIdType.MESH,
    )


def kernel(
    tok_hbm, wq_hbm, wl_hbm, gain_ref, wo_hbm, chosen_ref,
    out_ref, log_ref,
    tok_v, wq_v, wl_v, wo_v, own_v, sendbuf, table_ref, q_ref,
    req_v, reqin, idx_v, req_smem, idx_ref,
    kbuf, s_scr, m_scr, heads, stage, got,
    tok_sem, wq_sem, wl_sem, wo_sem, loc_sem, rs_sem, rr_sem, ds_sem, dr_sem,
    xs_sem, xl_sem, xr_sem, xd_sem, snd_sem, got_sem,
):
    me = lax.axis_index("kv")
    x = lax.axis_index("tp")
    mz = me // GRP
    myc = me % GRP
    left = (x + TP - 1) % TP
    right = (x + 1) % TP
    reqin[...] = jnp.zeros_like(reqin)
    barrier = pltpu.get_barrier_semaphore()

    @pl.loop(0, KV)
    def _(i):
        @pl.when(i != me)
        def _():
            pl.semaphore_signal(
                barrier, inc=1, device_id={"kv": i, "tp": x}, device_id_type=pl.DeviceIdType.MESH
            )

    for nb in (left, right):
        pl.semaphore_signal(
            barrier, inc=1, device_id={"kv": me, "tp": nb}, device_id_type=pl.DeviceIdType.MESH
        )

    def tok_copy(i):
        rows = pl.ds(i * 128, 128)
        return pltpu.make_async_copy(tok_hbm.at[rows], tok_v.at[rows], tok_sem.at[i])

    def wq_copy(h):
        cols = pl.ds(h * R, R)
        return pltpu.make_async_copy(wq_hbm.at[:, cols], wq_v.at[:, cols], wq_sem.at[h])

    wl_copy = pltpu.make_async_copy(wl_hbm, wl_v, wl_sem)
    wo_copy = pltpu.make_async_copy(wo_hbm, wo_v, wo_sem)
    wl_copy.start()
    for i in range(6):
        tok_copy(i).start()

    def hits(shape, g):
        c = jnp.broadcast_to(chosen_ref[g : g + 1, :].reshape((1,) * (len(shape) - 1) + (NSEL,)), shape)
        return c, ((c * 683) >> 13) == lax.broadcasted_iota(jnp.int32, shape, 0)

    far = jnp.full((KV, 1, NSEL), KV * PER, jnp.int32)
    near = jnp.full((KV, 1, NSEL), -1, jnp.int32)
    for g in range(PER):
        c, hit = hits((KV, 1, NSEL), g)
        far = jnp.minimum(far, jnp.where(hit, c, KV * PER))
        near = jnp.maximum(near, jnp.where(hit, c, -1))
    lo = jnp.min(far, axis=2, keepdims=True)
    hi = jnp.max(near, axis=2, keepdims=True)
    own0 = lax.broadcasted_iota(jnp.int32, (KV, 1, 1), 0) * PER
    pick = jnp.clip(jnp.where(x < 2, lo, hi) - own0, 0, PER - 1) * 2 + x % 2
    req_v[...] = jnp.broadcast_to(pick, req_v.shape)

    pl.semaphore_wait(barrier, KV - 1 + 2)

    def req_copy(i):
        return remote(req_v.at[i], reqin.at[me], rs_sem.at[i], rr_sem.at[me], i, x)

    @pl.loop(0, me)
    def _(i):
        req_copy(i).start()

    wl_copy.wait()
    for i in range(6):
        tok_copy(i).wait()
        p = jnp.dot(tok_v[i * 128 : (i + 1) * 128, :], wl_v[...], preferred_element_type=jnp.float32)
        inv = lax.rsqrt(jnp.mean(p * p, axis=-1, keepdims=True) + EPS)
        lat = (p * inv * gain_ref[...]).astype(jnp.bfloat16)
        own_v[4 * i : 4 * i + 4] = lat.reshape(4, HALF, R)
        table_ref[OWN + 4 * i : OWN + 4 * i + 4] = lat.reshape(4, HALF, R)

    for h in range(HEADS):
        wq_copy(h).start()
    wo_copy.start()

    @pl.loop(me + 1, KV)
    def _(i):
        remote(req_v.at[i], reqin.at[i], rs_sem.at[i], rr_sem.at[i], i, x).wait_recv()

    to_smem = pltpu.make_async_copy(reqin, req_smem, loc_sem)
    to_smem.start()
    to_smem.wait()

    def data_copy(d):
        return remote(
            sendbuf.at[d],
            table_ref.at[x * KV + me],
            ds_sem.at[d],
            dr_sem.at[jnp.where(d // GRP == mz, GRP + myc, mz)],
            d,
            x,
        )

    def each(delta, action):
        @pl.when(mz + delta < GRP)
        def _():
            @pl.loop(0, GRP)
            def _(k):
                d = (mz + delta) * GRP + (myc + k) % GRP

                @pl.when(d > me)
                def _():
                    action(d)

    def fill(d):
        sendbuf[d] = own_v[req_smem[d, 0, 0]]

    order = (7, 6, 4, 5, 3, 2, 1, 0)
    for s, delta in enumerate(order):
        each(delta, fill)
        if s >= 2:
            each(order[s - 2], lambda d: data_copy(d).wait_send())
        each(delta, lambda d: data_copy(d).start())

    far = jnp.full((KV, NSEL), KV * PER, jnp.int32)
    for g in range(PER):
        c, hit = hits((KV, NSEL), g)
        far = jnp.minimum(far, jnp.where(hit, c, KV * PER))
    lo = jnp.min(far, axis=1, keepdims=True)
    for g in range(PER):
        c, hit = hits((KV, NSEL), g)
        later = jnp.max(jnp.where(hit & (c > lo), 1, 0), axis=0, keepdims=True)
        c = chosen_ref[g : g + 1, :]
        owner = (c * 683) >> 13
        mine = owner == me
        valid = c >= 0
        first = jnp.where(mine, OWN + 2 * (c - me * PER), 2 * KV * later + owner)
        second = first + jnp.where(mine, 1, KV)
        idx_v[0, g : g + 1, 0:NSEL] = jnp.where(valid, first, OWN)
        idx_v[1, g : g + 1, 0:NSEL] = jnp.where(valid, second, OWN)
        live = jnp.sum(jnp.where(valid, 1, 0), axis=1, keepdims=True)
        idx_v[2, g : g + 1, :] = jnp.broadcast_to(live, (1, 128))
    idx_copy = pltpu.make_async_copy(idx_v, idx_ref, loc_sem)
    idx_copy.start()

    def region(quarter, z):
        return table_ref.at[pl.ds(quarter * KV + z * GRP, GRP)]

    def to_right(z):
        return remote(region(x, z), region(x, z), xs_sem.at[0, z], xl_sem.at[z], me, right)

    def to_left(z):
        return remote(region(x, z), region(x, z), xs_sem.at[1, z], xr_sem.at[z], me, left)

    def pass_right(z):
        return remote(region(left, z), region(left, z), xs_sem.at[2, z], xd_sem.at[z], me, right)

    def pass_left(z):
        return remote(region(right, z), region(right, z), xs_sem.at[2, z], xd_sem.at[z], me, left)

    near_first = (1, 2, 7, 3, 6, 5, 4)
    for dist in near_first:
        @pl.when(mz >= dist)
        def _(dist=dist):
            z = mz - dist
            pltpu.make_async_copy(region(x, z), region(x, z), dr_sem.at[z]).wait()
            to_right(z).start()
            to_left(z).start()

    @pl.when(myc > 0)
    def _():
        @pl.loop(0, myc)
        def _(k):
            one = table_ref.at[x * KV + mz * GRP + k]
            pltpu.make_async_copy(one, one, dr_sem.at[GRP + k]).wait()

        to_right(mz).start()
        to_left(mz).start()

    for h in range(HEADS):
        wq_copy(h).wait()
        q = jnp.dot(tok_v[...], wq_v[:, h * R : (h + 1) * R], preferred_element_type=jnp.float32)
        q_ref[:, h * R : (h + 1) * R] = (q.astype(jnp.bfloat16).astype(jnp.float32) * (R ** -0.5)).astype(jnp.bfloat16)

    for dist in near_first + (0,):
        z = mz - dist

        @pl.when((z >= 0) & ((dist != 0) | (myc > 0)))
        def _(z=z):
            to_right(z).wait_recv()
            to_left(z).wait_recv()

            @pl.when(z % 2 == 0)
            def _():
                pass_right(z).start()

            @pl.when(z % 2 == 1)
            def _():
                pass_left(z).start()

    idx_copy.wait()
    wo_copy.wait()
    for dist in near_first + (0,):
        z = mz - dist

        @pl.when((z >= 0) & ((dist != 0) | (myc > 0)))
        def _(z=z):
            pass_right(z).wait_recv()

    def dest(it):
        off = jnp.where(it == 0, 2, jnp.where(it == 1, 1, jnp.where(it == 2, 3, 0)))
        return (x + off) % TP

    rows = HEADS * BLK
    keys = NSEL * BLK
    step = 512

    def scores(b, slot):
        for j in range(2 * NSEL):
            kbuf[slot, j * HALF : (j + 1) * HALF, :] = table_ref[idx_ref[j % 2, b, j // 2]]
        here = pl.ds(pl.multiple_of(b * BLK, BLK), BLK)
        q = jnp.concatenate([q_ref[here, h * R : (h + 1) * R] for h in range(HEADS)], axis=0)
        live = idx_ref[2, b, 0] * BLK
        top = None
        for c in range(keys // step):
            s = lax.dot_general(
                q, kbuf[slot, c * step : (c + 1) * step, :], (((1,), (1,)), ((), ())),
                preferred_element_type=jnp.float32,
            )
            col = lax.broadcasted_iota(jnp.int32, (rows, step), 1)
            ok = col + c * step < live
            if c == 0:
                t = lax.broadcasted_iota(jnp.int32, (rows, step), 0) % BLK
                ok = ok & ((col >= BLK) | (col <= t))
            s = jnp.where(ok, s, -jnp.inf)
            s_scr[slot, :, c * step : (c + 1) * step] = s
            for k in range(step // 128):
                part = s[:, k * 128 : (k + 1) * 128]
                top = part if top is None else jnp.maximum(top, part)
        m_scr[slot] = top

    def values(b, slot, j):
        peak = jnp.max(m_scr[slot], axis=1, keepdims=True)
        total = None
        o = None
        for c in range(keys // step):
            e = jnp.exp(s_scr[slot, :, c * step : (c + 1) * step] - peak)
            for k in range(step // 128):
                part = e[:, k * 128 : (k + 1) * 128]
                total = part if total is None else total + part
            oc = jnp.dot(
                e.astype(jnp.bfloat16), kbuf[slot, c * step : (c + 1) * step, :],
                preferred_element_type=jnp.float32,
            )
            o = oc if o is None else o + oc
        mass = jnp.sum(total, axis=1, keepdims=True)
        o = o / mass
        logs = peak + jnp.log(mass)
        here = pl.ds(pl.multiple_of(b * BLK, BLK), BLK)
        for h in range(HEADS):
            heads[j * BLK : (j + 1) * BLK, h * R : (h + 1) * R] = o[h * BLK : (h + 1) * BLK].astype(jnp.bfloat16)
            log_ref[here, h : h + 1] = logs[h * BLK : (h + 1) * BLK]

    def move(k):
        src, slot, nb = (
            (stage.at[0, 0], 0, right),
            (stage.at[0, 1], 1, left),
            (stage.at[1, 1], 2, right),
            (stage.at[2, 0], 3, left),
            (stage.at[1, 0], 4, right),
            (stage.at[2, 1], 5, left),
        )[k]
        return remote(src, got.at[slot], snd_sem.at[k], got_sem.at[slot], me, nb)

    scores(3 * dest(0), 0)

    @pl.loop(0, TP)
    def _(it):
        b0 = 3 * dest(it)
        nxt = jnp.where(it == TP - 1, b0, 3 * dest(it + 1))
        for j in range(3):
            scores(b0 + j + 1 if j < 2 else nxt, (j + 1) % 3)
            values(b0 + j, j, j)
        for n in range(8):
            part = jnp.dot(heads[...], wo_v[:, n * 256 : (n + 1) * 256], preferred_element_type=jnp.float32)
            stage[it, n // 4, :, (n % 4) * 256 : (n % 4 + 1) * 256] = part.astype(jnp.bfloat16)

        @pl.when(it == 0)
        def _():
            move(0).start()
            move(1).start()

        @pl.when(it == 1)
        def _():
            move(2).start()

        @pl.when(it == 2)
        def _():
            move(3).start()

    f32 = jnp.float32
    move(0).wait_recv()
    stage[1, 0] = (stage[1, 0].astype(f32) + got[0].astype(f32)).astype(jnp.bfloat16)
    move(4).start()
    move(1).wait_recv()
    stage[2, 1] = (stage[2, 1].astype(f32) + got[1].astype(f32)).astype(jnp.bfloat16)
    move(5).start()
    half = 1024
    for k, h in ((0, 0), (1, 1)):
        move(3 - k).wait_recv()
        move(4 + k).wait_recv()
        lo = 3 if h == 0 else 2
        hi = 4 if h == 0 else 5
        total = stage[3, h].astype(f32) + got[lo].astype(f32) + got[hi].astype(f32)
        out_ref[:, h * half : (h + 1) * half] = total.astype(jnp.bfloat16)
    for k in range(6):
        move(k).wait_send()

    for dist in near_first + (0,):
        z = mz - dist

        @pl.when((z >= 0) & ((dist != 0) | (myc > 0)))
        def _(z=z):
            to_right(z).wait_send()
            to_left(z).wait_send()
            pass_right(z).wait_send()

    for delta in order[-2:]:
        each(delta, lambda d: data_copy(d).wait_send())

    @pl.loop(0, me)
    def _(i):
        req_copy(i).wait_send()


def local(tokens, w_query, w_latent, latent_gain, w_output, chosen):
    vmem = pl.BlockSpec(memory_space=pltpu.VMEM)
    hbm = pl.BlockSpec(memory_space=pltpu.HBM)
    dma = pltpu.SemaphoreType.DMA
    bf16 = jnp.bfloat16
    part = ROWS // TP
    return pl.pallas_call(
        kernel,
        out_shape=(
            jax.ShapeDtypeStruct((part, 2048), bf16),
            jax.ShapeDtypeStruct((ROWS, HEADS), jnp.float32),
        ),
        in_specs=[hbm, hbm, hbm, vmem, hbm, vmem],
        out_specs=(vmem, vmem),
        scratch_shapes=[
            pltpu.VMEM(tokens.shape, bf16),
            pltpu.VMEM(w_query.shape, bf16),
            pltpu.VMEM(w_latent.shape, bf16),
            pltpu.VMEM(w_output.shape, bf16),
            pltpu.VMEM((2 * PER, HALF, R), bf16),
            pltpu.VMEM((KV, HALF, R), bf16),
            pltpu.VMEM((SLOTS, HALF, R), bf16),
            pltpu.VMEM((ROWS, HEADS * R), bf16),
            pltpu.VMEM((KV, 1, 128), jnp.int32),
            pltpu.VMEM((KV, 1, 128), jnp.int32),
            pltpu.VMEM((3, 16, 128), jnp.int32),
            pltpu.SMEM((KV, 1, 128), jnp.int32),
            pltpu.SMEM((3, 16, 128), jnp.int32),
            pltpu.VMEM((3, NSEL * BLK, R), bf16),
            pltpu.VMEM((3, HEADS * BLK, NSEL * BLK), jnp.float32),
            pltpu.VMEM((3, HEADS * BLK, 128), jnp.float32),
            pltpu.VMEM((part, HEADS * R), bf16),
            pltpu.VMEM((TP, 2, part, 1024), bf16),
            pltpu.VMEM((6, part, 1024), bf16),
            dma((6,)),
            dma((HEADS,)),
            dma,
            dma,
            dma,
            dma((KV,)),
            dma((KV,)),
            dma((KV,)),
            dma((2 * GRP,)),
            dma((3, GRP)),
            dma((GRP,)),
            dma((GRP,)),
            dma((GRP,)),
            dma((6,)),
            dma((6,)),
        ],
        compiler_params=pltpu.CompilerParams(
            collective_id=0, has_side_effects=True, vmem_limit_bytes=60 * 1024 * 1024
        ),
        name="layer",
    )(tokens, w_query, w_latent, latent_gain.reshape(1, R), w_output, chosen)


def solution(mesh):
    placed = (P("kv", None), P(None, "tp"), P(), P(), P("tp", None), P("kv", None))
    return jax.shard_map(
        local,
        mesh=mesh,
        in_specs=placed,
        out_specs=(P(("kv", "tp"), None), P("kv", "tp")),
        check_vma=False,
    )
```

```python
import functools

import jax
import jax.numpy as jnp
from jax import lax
from jax.experimental import pallas as pl
from jax.experimental.pallas import tpu as pltpu
from jax.sharding import PartitionSpec as P

EPS = 1e-06
KV = 64
TP = 4
GRP = 8
BLK = 64
HALF = 32
R = 256
PER = 12
NSEL = 32
OWN = TP * KV
SLOTS = OWN + 2 * PER
ROWS = PER * BLK
HEADS = 4


def remote(src, dst, send_sem, recv_sem, kv, tp):
    return pltpu.make_async_remote_copy(
        src_ref=src,
        dst_ref=dst,
        send_sem=send_sem,
        recv_sem=recv_sem,
        device_id={"kv": kv, "tp": tp},
        device_id_type=pl.DeviceIdType.MESH,
    )


def kernel(
    tok_hbm, wq_hbm, wl_hbm, gain_ref, wo_hbm, chosen_ref,
    out_ref, log_ref,
    tok_v, wq_v, wl_v, wo_v, own_v, sendbuf, table_ref, q_ref,
    req_v, reqin, idx_v, req_smem, idx_ref,
    kbuf, s_scr, m_scr, heads, stage, got, log_v,
    tok_sem, wq_sem, wl_sem, wo_sem, loc_sem, rs_sem, rr_sem, ds_sem, dr_sem,
    xs_sem, xl_sem, xr_sem, xd_sem, snd_sem, got_sem,
):
    me = lax.axis_index("kv")
    x = lax.axis_index("tp")
    mz = me // GRP
    myc = me % GRP
    left = (x + TP - 1) % TP
    right = (x + 1) % TP
    reqin[...] = jnp.zeros_like(reqin)
    barrier = pltpu.get_barrier_semaphore()

    @pl.loop(0, KV)
    def _(i):
        @pl.when(i != me)
        def _():
            pl.semaphore_signal(
                barrier, inc=1, device_id={"kv": i, "tp": x}, device_id_type=pl.DeviceIdType.MESH
            )

    for nb in (left, right):
        pl.semaphore_signal(
            barrier, inc=1, device_id={"kv": me, "tp": nb}, device_id_type=pl.DeviceIdType.MESH
        )

    def tok_copy(i):
        rows = pl.ds(i * 128, 128)
        return pltpu.make_async_copy(tok_hbm.at[rows], tok_v.at[rows], tok_sem.at[i])

    def wq_copy(h):
        cols = pl.ds(h * R, R)
        return pltpu.make_async_copy(wq_hbm.at[:, cols], wq_v.at[:, cols], wq_sem.at[h])

    wl_copy = pltpu.make_async_copy(wl_hbm, wl_v, wl_sem)
    wo_copy = pltpu.make_async_copy(wo_hbm, wo_v, wo_sem)
    wl_copy.start()
    for i in range(6):
        tok_copy(i).start()

    def hits(shape, g):
        c = jnp.broadcast_to(chosen_ref[g : g + 1, :].reshape((1,) * (len(shape) - 1) + (NSEL,)), shape)
        return c, ((c * 683) >> 13) == lax.broadcasted_iota(jnp.int32, shape, 0)

    far = jnp.full((KV, 1, NSEL), KV * PER, jnp.int32)
    near = jnp.full((KV, 1, NSEL), -1, jnp.int32)
    for g in range(PER):
        c, hit = hits((KV, 1, NSEL), g)
        far = jnp.minimum(far, jnp.where(hit, c, KV * PER))
        near = jnp.maximum(near, jnp.where(hit, c, -1))
    lo = jnp.min(far, axis=2, keepdims=True)
    hi = jnp.max(near, axis=2, keepdims=True)
    own0 = lax.broadcasted_iota(jnp.int32, (KV, 1, 1), 0) * PER
    pick = jnp.clip(jnp.where(x < 2, lo, hi) - own0, 0, PER - 1) * 2 + x % 2
    req_v[...] = jnp.broadcast_to(pick, req_v.shape)

    pl.semaphore_wait(barrier, KV - 1 + 2)

    def req_copy(i):
        return remote(req_v.at[i], reqin.at[me], rs_sem.at[i], rr_sem.at[me], i, x)

    @pl.loop(0, me)
    def _(i):
        req_copy(i).start()

    wl_copy.wait()
    for i in range(6):
        tok_copy(i).wait()
        p = jnp.dot(tok_v[i * 128 : (i + 1) * 128, :], wl_v[...], preferred_element_type=jnp.float32)
        inv = lax.rsqrt(jnp.mean(p * p, axis=-1, keepdims=True) + EPS)
        lat = (p * inv * gain_ref[...]).astype(jnp.bfloat16)
        own_v[4 * i : 4 * i + 4] = lat.reshape(4, HALF, R)
        table_ref[OWN + 4 * i : OWN + 4 * i + 4] = lat.reshape(4, HALF, R)

    for h in range(HEADS):
        wq_copy(h).start()
    wo_copy.start()

    @pl.loop(me + 1, KV)
    def _(i):
        remote(req_v.at[i], reqin.at[i], rs_sem.at[i], rr_sem.at[i], i, x).wait_recv()

    to_smem = pltpu.make_async_copy(reqin, req_smem, loc_sem)
    to_smem.start()
    to_smem.wait()

    def data_copy(d):
        return remote(
            sendbuf.at[d],
            table_ref.at[x * KV + me],
            ds_sem.at[d],
            dr_sem.at[jnp.where(d // GRP == mz, GRP + myc, mz)],
            d,
            x,
        )

    def each(delta, action):
        @pl.when(mz + delta < GRP)
        def _():
            @pl.loop(0, GRP)
            def _(k):
                d = (mz + delta) * GRP + (myc + k) % GRP

                @pl.when(d > me)
                def _():
                    action(d)

    def fill(d):
        sendbuf[d] = own_v[req_smem[d, 0, 0]]

    order = (0, 1, 7, 2, 6, 3, 5, 4)

    def send_group(s):
        each(order[s], fill)
        if s >= 3:
            each(order[s - 2], lambda d: data_copy(d).wait_send())
        each(order[s], lambda d: data_copy(d).start())

    def project_query(h):
        wq_copy(h).wait()
        q = jnp.dot(tok_v[...], wq_v[:, h * R : (h + 1) * R], preferred_element_type=jnp.float32)
        q_ref[:, h * R : (h + 1) * R] = (q.astype(jnp.bfloat16).astype(jnp.float32) * (R ** -0.5)).astype(jnp.bfloat16)

    def region(quarter, z):
        return table_ref.at[pl.ds(quarter * KV + z * GRP, GRP)]

    def to_right(z):
        return remote(region(x, z), region(x, z), xs_sem.at[0, z], xl_sem.at[z], me, right)

    def to_left(z):
        return remote(region(x, z), region(x, z), xs_sem.at[1, z], xr_sem.at[z], me, left)

    def pass_right(z):
        return remote(region(left, z), region(left, z), xs_sem.at[2, z], xd_sem.at[z], me, right)

    def pass_left(z):
        return remote(region(right, z), region(right, z), xs_sem.at[2, z], xd_sem.at[z], me, left)

    send_group(0)
    send_group(1)
    send_group(2)
    project_query(0)
    project_query(1)
    @pl.when(myc > 0)
    def _():
        @pl.loop(0, myc)
        def _(k):
            one = table_ref.at[x * KV + mz * GRP + k]
            pltpu.make_async_copy(one, one, dr_sem.at[GRP + k]).wait()

        to_right(mz).start()
        to_left(mz).start()

    send_group(3)
    project_query(2)
    send_group(4)
    project_query(3)
    far = jnp.full((KV, NSEL), KV * PER, jnp.int32)
    for g in range(PER):
        c, hit = hits((KV, NSEL), g)
        far = jnp.minimum(far, jnp.where(hit, c, KV * PER))
    lo = jnp.min(far, axis=1, keepdims=True)
    for g in range(PER):
        c, hit = hits((KV, NSEL), g)
        later = jnp.max(jnp.where(hit & (c > lo), 1, 0), axis=0, keepdims=True)
        c = chosen_ref[g : g + 1, :]
        owner = (c * 683) >> 13
        mine = owner == me
        valid = c >= 0
        first = jnp.where(mine, OWN + 2 * (c - me * PER), 2 * KV * later + owner)
        second = first + jnp.where(mine, 1, KV)
        idx_v[0, g : g + 1, 0:NSEL] = jnp.where(valid, first, OWN)
        idx_v[1, g : g + 1, 0:NSEL] = jnp.where(valid, second, OWN)
        live = jnp.sum(jnp.where(valid, 1, 0), axis=1, keepdims=True)
        idx_v[2, g : g + 1, :] = jnp.broadcast_to(live, (1, 128))
    idx_copy = pltpu.make_async_copy(idx_v, idx_ref, loc_sem)
    idx_copy.start()

    dists = (0, 1, 7, 2, 6, 3, 5, 4)

    def have(dist):
        return (mz >= dist) if dist else (myc > 0)

    def share(dist):
        @pl.when(mz >= dist)
        def _():
            z = mz - dist
            pltpu.make_async_copy(region(x, z), region(x, z), dr_sem.at[z]).wait()
            to_right(z).start()
            to_left(z).start()

    def relay(dist):
        @pl.when(have(dist))
        def _():
            z = mz - dist
            to_right(z).wait_recv()
            to_left(z).wait_recv()

            @pl.when(z % 2 == 0)
            def _():
                pass_right(z).start()

            @pl.when(z % 2 == 1)
            def _():
                pass_left(z).start()

    share(1)
    send_group(5)
    share(7)
    relay(0)
    send_group(6)
    share(2)
    relay(1)
    send_group(7)
    share(6)
    relay(7)
    share(3)
    relay(2)
    share(5)
    relay(6)
    share(4)
    relay(3)
    relay(5)
    relay(4)

    idx_copy.wait()
    wo_copy.wait()
    for dist in dists:
        z = mz - dist

        @pl.when(have(dist))
        def _(z=z):
            pass_right(z).wait_recv()

    def dest(it):
        off = jnp.where(it == 0, 2, jnp.where(it == 1, 1, jnp.where(it == 2, 3, 0)))
        return (x + off) % TP

    rows = HEADS * BLK
    keys = NSEL * BLK
    step = 512

    def scores(b, slot):
        for j in range(2 * NSEL):
            kbuf[slot, j * HALF : (j + 1) * HALF, :] = table_ref[idx_ref[j % 2, b, j // 2]]
        here = pl.ds(pl.multiple_of(b * BLK, BLK), BLK)
        q = jnp.concatenate([q_ref[here, h * R : (h + 1) * R] for h in range(HEADS)], axis=0)
        live = idx_ref[2, b, 0] * BLK
        top = None
        for c in range(keys // step):
            s = lax.dot_general(
                q, kbuf[slot, c * step : (c + 1) * step, :], (((1,), (1,)), ((), ())),
                preferred_element_type=jnp.float32,
            )
            col = lax.broadcasted_iota(jnp.int32, (rows, step), 1)
            ok = col + c * step < live
            if c == 0:
                t = lax.broadcasted_iota(jnp.int32, (rows, step), 0) % BLK
                ok = ok & ((col >= BLK) | (col <= t))
            s = jnp.where(ok, s, -jnp.inf)
            s_scr[slot, :, c * step : (c + 1) * step] = s
            for k in range(step // 128):
                part = s[:, k * 128 : (k + 1) * 128]
                top = part if top is None else jnp.maximum(top, part)
        m_scr[slot] = top

    def values(b, slot, j):
        peak = jnp.max(m_scr[slot], axis=1, keepdims=True)
        total = None
        o = None
        for c in range(keys // step):
            e = jnp.exp(s_scr[slot, :, c * step : (c + 1) * step] - peak)
            for k in range(step // 128):
                part = e[:, k * 128 : (k + 1) * 128]
                total = part if total is None else total + part
            oc = jnp.dot(
                e.astype(jnp.bfloat16), kbuf[slot, c * step : (c + 1) * step, :],
                preferred_element_type=jnp.float32,
            )
            o = oc if o is None else o + oc
        mass = jnp.sum(total, axis=1, keepdims=True)
        o = o / mass
        logs = peak + jnp.log(mass)
        here = pl.ds(pl.multiple_of(b * BLK, BLK), BLK)
        for h in range(HEADS):
            heads[j * BLK : (j + 1) * BLK, h * R : (h + 1) * R] = o[h * BLK : (h + 1) * BLK].astype(jnp.bfloat16)
            log_v[here, h : h + 1] = logs[h * BLK : (h + 1) * BLK]

    half = 1024
    quarter = 256

    def project(it, lo, hi):
        for n in range(2048 // quarter):
            part = jnp.dot(
                heads[lo:hi, :], wo_v[:, n * quarter : (n + 1) * quarter], preferred_element_type=jnp.float32
            )
            c = n * quarter % half
            stage[it, n * quarter // half, lo:hi, c : c + quarter] = part.astype(jnp.bfloat16)

    def first(h):
        return remote(stage.at[0, h], got.at[h], snd_sem.at[h], got_sem.at[h], me, right if h == 0 else left)

    def move(k):
        it, h, nb = ((1, 1, right), (2, 0, left), (1, 0, right), (2, 1, left))[k]
        return remote(stage.at[it, h], got.at[2 + k], snd_sem.at[2 + k], got_sem.at[2 + k], me, nb)

    scores(3 * dest(0), 0)

    @pl.loop(0, TP)
    def _(it):
        b0 = 3 * dest(it)
        nxt = jnp.where(it == TP - 1, b0, 3 * dest(it + 1))
        for j in range(3):
            scores(b0 + j + 1 if j < 2 else nxt, (j + 1) % 3)
            values(b0 + j, j, j)
        project(it, 0, 3 * BLK)

        @pl.when(it == 0)
        def _():
            first(0).start()
            first(1).start()

        @pl.when(it == 1)
        def _():
            move(0).start()

        @pl.when(it == 2)
        def _():
            move(1).start()

    f32 = jnp.float32
    for h in range(2):
        first(h).wait_recv()
        stage[1 + h, h] = (stage[1 + h, h].astype(f32) + got[h].astype(f32)).astype(jnp.bfloat16)
        move(2 + h).start()
    log_ref[...] = jnp.transpose(log_v[...])[0:HEADS]
    for h in range(2):
        move(1 - h).wait_recv()
        move(2 + h).wait_recv()
        total = stage[3, h].astype(f32) + got[3 - h].astype(f32) + got[4 + h].astype(f32)
        out_ref[:, h * half : (h + 1) * half] = total.astype(jnp.bfloat16)
    for h in range(2):
        first(h).wait_send()
    for k in range(4):
        move(k).wait_send()

    for dist in dists:
        z = mz - dist

        @pl.when(have(dist))
        def _(z=z):
            to_right(z).wait_send()
            to_left(z).wait_send()
            pass_right(z).wait_send()

    for delta in order[:1] + order[-2:]:
        each(delta, lambda d: data_copy(d).wait_send())

    @pl.loop(0, me)
    def _(i):
        req_copy(i).wait_send()


def local(tokens, w_query, w_latent, latent_gain, w_output, chosen):
    vmem = pl.BlockSpec(memory_space=pltpu.VMEM)
    hbm = pl.BlockSpec(memory_space=pltpu.HBM)
    dma = pltpu.SemaphoreType.DMA
    bf16 = jnp.bfloat16
    part = ROWS // TP
    attended, logs = pl.pallas_call(
        kernel,
        out_shape=(
            jax.ShapeDtypeStruct((part, 2048), bf16),
            jax.ShapeDtypeStruct((HEADS, ROWS), jnp.float32),
        ),
        in_specs=[hbm, hbm, hbm, vmem, hbm, vmem],
        out_specs=(vmem, vmem),
        scratch_shapes=[
            pltpu.VMEM(tokens.shape, bf16),
            pltpu.VMEM(w_query.shape, bf16),
            pltpu.VMEM(w_latent.shape, bf16),
            pltpu.VMEM(w_output.shape, bf16),
            pltpu.VMEM((2 * PER, HALF, R), bf16),
            pltpu.VMEM((KV, HALF, R), bf16),
            pltpu.VMEM((SLOTS, HALF, R), bf16),
            pltpu.VMEM((ROWS, HEADS * R), bf16),
            pltpu.VMEM((KV, 1, 128), jnp.int32),
            pltpu.VMEM((KV, 1, 128), jnp.int32),
            pltpu.VMEM((3, 16, 128), jnp.int32),
            pltpu.SMEM((KV, 1, 128), jnp.int32),
            pltpu.SMEM((3, 16, 128), jnp.int32),
            pltpu.VMEM((3, NSEL * BLK, R), bf16),
            pltpu.VMEM((3, HEADS * BLK, NSEL * BLK), jnp.float32),
            pltpu.VMEM((3, HEADS * BLK, 128), jnp.float32),
            pltpu.VMEM((part, HEADS * R), bf16),
            pltpu.VMEM((TP, 2, part, 1024), bf16),
            pltpu.VMEM((6, part, 1024), bf16),
            pltpu.VMEM((ROWS, 128), jnp.float32),
            dma((6,)),
            dma((HEADS,)),
            dma,
            dma,
            dma,
            dma((KV,)),
            dma((KV,)),
            dma((KV,)),
            dma((2 * GRP,)),
            dma((3, GRP)),
            dma((GRP,)),
            dma((GRP,)),
            dma((GRP,)),
            dma((6,)),
            dma((6,)),
        ],
        compiler_params=pltpu.CompilerParams(
            collective_id=0, has_side_effects=True, vmem_limit_bytes=53 * 1024 * 1024
        ),
        name="layer",
    )(tokens, w_query, w_latent, latent_gain.reshape(1, R), w_output, chosen)
    return attended, logs.T


def solution(mesh):
    placed = (P("kv", None), P(None, "tp"), P(), P(), P("tp", None), P("kv", None))
    return jax.shard_map(
        local,
        mesh=mesh,
        in_specs=placed,
        out_specs=(P(("kv", "tp"), None), P("kv", "tp")),
        check_vma=False,
    )
```

```python
import functools

import jax
import jax.numpy as jnp
from jax import lax
from jax.experimental import pallas as pl
from jax.experimental.pallas import tpu as pltpu
from jax.sharding import PartitionSpec as P

EPS = 1e-06
KV = 64
TP = 4
GRP = 8
BLK = 64
HALF = 32
R = 256
PER = 12
NSEL = 32
OWN = TP * KV
SLOTS = OWN + 2 * PER
ROWS = PER * BLK
HEADS = 4


def remote(src, dst, send_sem, recv_sem, kv, tp):
    return pltpu.make_async_remote_copy(
        src_ref=src,
        dst_ref=dst,
        send_sem=send_sem,
        recv_sem=recv_sem,
        device_id={"kv": kv, "tp": tp},
        device_id_type=pl.DeviceIdType.MESH,
    )


def kernel(
    tok_hbm, wq_hbm, wl_hbm, gain_ref, wo_hbm, chosen_ref,
    out_ref, log_ref,
    tok_v, wq_v, wl_v, wo_v, own_v, sendbuf, table_ref, q_ref,
    req_v, reqin, idx_v, req_smem, idx_ref,
    kbuf, s_scr, m_scr, heads, stage, got, log_v,
    tok_sem, wq_sem, wl_sem, wo_sem, loc_sem, rs_sem, rr_sem, ds_sem, dr_sem,
    xs_sem, xl_sem, xr_sem, xd_sem, snd_sem, got_sem,
):
    me = lax.axis_index("kv")
    x = lax.axis_index("tp")
    mz = me // GRP
    myc = me % GRP
    left = (x + TP - 1) % TP
    right = (x + 1) % TP
    reqin[...] = jnp.zeros_like(reqin)
    barrier = pltpu.get_barrier_semaphore()

    @pl.loop(0, KV)
    def _(i):
        @pl.when(i != me)
        def _():
            pl.semaphore_signal(
                barrier, inc=1, device_id={"kv": i, "tp": x}, device_id_type=pl.DeviceIdType.MESH
            )

    for nb in (left, right):
        pl.semaphore_signal(
            barrier, inc=1, device_id={"kv": me, "tp": nb}, device_id_type=pl.DeviceIdType.MESH
        )

    def tok_copy(i):
        rows = pl.ds(i * 128, 128)
        return pltpu.make_async_copy(tok_hbm.at[rows], tok_v.at[rows], tok_sem.at[i])

    def wq_copy(h):
        cols = pl.ds(h * R, R)
        return pltpu.make_async_copy(wq_hbm.at[:, cols], wq_v.at[:, cols], wq_sem.at[h])

    wl_copy = pltpu.make_async_copy(wl_hbm, wl_v, wl_sem)
    wo_copy = pltpu.make_async_copy(wo_hbm, wo_v, wo_sem)
    wl_copy.start()
    for i in range(6):
        tok_copy(i).start()

    def hits(shape, g):
        c = jnp.broadcast_to(chosen_ref[g : g + 1, :].reshape((1,) * (len(shape) - 1) + (NSEL,)), shape)
        return c, ((c * 683) >> 13) == lax.broadcasted_iota(jnp.int32, shape, 0)

    far = jnp.full((KV, 1, NSEL), KV * PER, jnp.int32)
    near = jnp.full((KV, 1, NSEL), -1, jnp.int32)
    for g in range(PER):
        c, hit = hits((KV, 1, NSEL), g)
        far = jnp.minimum(far, jnp.where(hit, c, KV * PER))
        near = jnp.maximum(near, jnp.where(hit, c, -1))
    lo = jnp.min(far, axis=2, keepdims=True)
    hi = jnp.max(near, axis=2, keepdims=True)
    own0 = lax.broadcasted_iota(jnp.int32, (KV, 1, 1), 0) * PER
    pick = jnp.clip(jnp.where(x < 2, lo, hi) - own0, 0, PER - 1) * 2 + x % 2
    req_v[...] = jnp.broadcast_to(pick, req_v.shape)

    pl.semaphore_wait(barrier, KV - 1 + 2)

    def req_copy(i):
        return remote(req_v.at[i], reqin.at[me], rs_sem.at[i], rr_sem.at[me], i, x)

    @pl.loop(0, me)
    def _(i):
        req_copy(i).start()

    wl_copy.wait()
    for i in range(6):
        tok_copy(i).wait()
        p = jnp.dot(tok_v[i * 128 : (i + 1) * 128, :], wl_v[...], preferred_element_type=jnp.float32)
        inv = lax.rsqrt(jnp.mean(p * p, axis=-1, keepdims=True) + EPS)
        lat = (p * inv * gain_ref[...]).astype(jnp.bfloat16)
        own_v[4 * i : 4 * i + 4] = lat.reshape(4, HALF, R)
        table_ref[OWN + 4 * i : OWN + 4 * i + 4] = lat.reshape(4, HALF, R)

    for h in range(HEADS):
        wq_copy(h).start()
    wo_copy.start()

    @pl.loop(me + 1, KV)
    def _(i):
        remote(req_v.at[i], reqin.at[i], rs_sem.at[i], rr_sem.at[i], i, x).wait_recv()

    to_smem = pltpu.make_async_copy(reqin, req_smem, loc_sem)
    to_smem.start()
    to_smem.wait()

    def data_copy(d):
        return remote(
            sendbuf.at[d],
            table_ref.at[x * KV + me],
            ds_sem.at[d],
            dr_sem.at[jnp.where(d // GRP == mz, GRP + myc, mz)],
            d,
            x,
        )

    def each(delta, action):
        @pl.when(mz + delta < GRP)
        def _():
            @pl.loop(0, GRP)
            def _(k):
                d = (mz + delta) * GRP + (myc + k) % GRP

                @pl.when(d > me)
                def _():
                    action(d)

    def fill(d):
        sendbuf[d] = own_v[req_smem[d, 0, 0]]

    order = (0, 1, 7, 2, 6, 3, 5, 4)

    def send_group(s):
        each(order[s], fill)
        if s >= 5:
            each(order[s - 4], lambda d: data_copy(d).wait_send())
        each(order[s], lambda d: data_copy(d).start())

    def project_query(h):
        wq_copy(h).wait()
        q = jnp.dot(tok_v[...], wq_v[:, h * R : (h + 1) * R], preferred_element_type=jnp.float32)
        q_ref[:, h * R : (h + 1) * R] = (q.astype(jnp.bfloat16).astype(jnp.float32) * (R ** -0.5)).astype(jnp.bfloat16)

    def region(quarter, z):
        return table_ref.at[pl.ds(quarter * KV + z * GRP, GRP)]

    def to_right(z):
        return remote(region(x, z), region(x, z), xs_sem.at[0, z], xl_sem.at[z], me, right)

    def to_left(z):
        return remote(region(x, z), region(x, z), xs_sem.at[1, z], xr_sem.at[z], me, left)

    def pass_right(z):
        return remote(region(left, z), region(left, z), xs_sem.at[2, z], xd_sem.at[z], me, right)

    def pass_left(z):
        return remote(region(right, z), region(right, z), xs_sem.at[2, z], xd_sem.at[z], me, left)

    for s in range(5):
        send_group(s)
    project_query(0)
    project_query(1)

    @pl.when(myc > 0)
    def _():
        @pl.loop(0, myc)
        def _(k):
            one = table_ref.at[x * KV + mz * GRP + k]
            pltpu.make_async_copy(one, one, dr_sem.at[GRP + k]).wait()

        to_right(mz).start()
        to_left(mz).start()

    send_group(5)
    project_query(2)
    send_group(6)
    project_query(3)
    send_group(7)
    far = jnp.full((KV, NSEL), KV * PER, jnp.int32)
    for g in range(PER):
        c, hit = hits((KV, NSEL), g)
        far = jnp.minimum(far, jnp.where(hit, c, KV * PER))
    lo = jnp.min(far, axis=1, keepdims=True)
    for g in range(PER):
        c, hit = hits((KV, NSEL), g)
        later = jnp.max(jnp.where(hit & (c > lo), 1, 0), axis=0, keepdims=True)
        c = chosen_ref[g : g + 1, :]
        owner = (c * 683) >> 13
        mine = owner == me
        valid = c >= 0
        first = jnp.where(mine, OWN + 2 * (c - me * PER), 2 * KV * later + owner)
        second = first + jnp.where(mine, 1, KV)
        idx_v[0, g : g + 1, 0:NSEL] = jnp.where(valid, first, OWN)
        idx_v[1, g : g + 1, 0:NSEL] = jnp.where(valid, second, OWN)
        live = jnp.sum(jnp.where(valid, 1, 0), axis=1, keepdims=True)
        idx_v[2, g : g + 1, :] = jnp.broadcast_to(live, (1, 128))
    idx_copy = pltpu.make_async_copy(idx_v, idx_ref, loc_sem)
    idx_copy.start()

    dists = (0, 1, 7, 2, 6, 3, 5, 4)

    def have(dist):
        return (mz >= dist) if dist else (myc > 0)

    def share(dist, only=None):
        @pl.when((mz >= dist) if only is None else (mz == only))
        def _():
            z = mz - dist
            pltpu.make_async_copy(region(x, z), region(x, z), dr_sem.at[z]).wait()
            to_right(z).start()
            to_left(z).start()

    def relay(dist):
        @pl.when(have(dist))
        def _():
            z = mz - dist
            to_right(z).wait_recv()
            to_left(z).wait_recv()

            @pl.when(z % 2 == 0)
            def _():
                pass_right(z).start()

            @pl.when(z % 2 == 1)
            def _():
                pass_left(z).start()

    share(1)
    share(7)
    relay(0)
    share(2)
    relay(1)
    relay(7)
    share(6, GRP - 1)
    share(3)
    relay(2)
    share(6, 6)
    share(5)
    relay(6)
    relay(3)
    share(4)
    relay(5)
    relay(4)

    idx_copy.wait()
    wo_copy.wait()
    for dist in dists:
        z = mz - dist

        @pl.when(have(dist))
        def _(z=z):
            pass_right(z).wait_recv()

    def dest(it):
        off = jnp.where(it == 0, 2, jnp.where(it == 1, 1, jnp.where(it == 2, 3, 0)))
        return (x + off) % TP

    rows = HEADS * BLK
    keys = NSEL * BLK
    step = 512

    def scores(b, slot):
        for j in range(2 * NSEL):
            kbuf[slot, j * HALF : (j + 1) * HALF, :] = table_ref[idx_ref[j % 2, b, j // 2]]
        here = pl.ds(pl.multiple_of(b * BLK, BLK), BLK)
        q = jnp.concatenate([q_ref[here, h * R : (h + 1) * R] for h in range(HEADS)], axis=0)
        live = idx_ref[2, b, 0] * BLK
        top = None
        for c in range(keys // step):
            s = lax.dot_general(
                q, kbuf[slot, c * step : (c + 1) * step, :], (((1,), (1,)), ((), ())),
                preferred_element_type=jnp.float32,
            )
            col = lax.broadcasted_iota(jnp.int32, (rows, step), 1)
            ok = col + c * step < live
            if c == 0:
                t = lax.broadcasted_iota(jnp.int32, (rows, step), 0) % BLK
                ok = ok & ((col >= BLK) | (col <= t))
            s = jnp.where(ok, s, -jnp.inf)
            s_scr[slot, :, c * step : (c + 1) * step] = s
            for k in range(step // 128):
                part = s[:, k * 128 : (k + 1) * 128]
                top = part if top is None else jnp.maximum(top, part)
        m_scr[slot] = top

    def values(b, slot, j):
        peak = jnp.max(m_scr[slot], axis=1, keepdims=True)
        total = None
        o = None
        for c in range(keys // step):
            e = jnp.exp(s_scr[slot, :, c * step : (c + 1) * step] - peak)
            for k in range(step // 128):
                part = e[:, k * 128 : (k + 1) * 128]
                total = part if total is None else total + part
            oc = jnp.dot(
                e.astype(jnp.bfloat16), kbuf[slot, c * step : (c + 1) * step, :],
                preferred_element_type=jnp.float32,
            )
            o = oc if o is None else o + oc
        mass = jnp.sum(total, axis=1, keepdims=True)
        o = o / mass
        logs = peak + jnp.log(mass)
        here = pl.ds(pl.multiple_of(b * BLK, BLK), BLK)
        for h in range(HEADS):
            heads[j * BLK : (j + 1) * BLK, h * R : (h + 1) * R] = o[h * BLK : (h + 1) * BLK].astype(jnp.bfloat16)
            log_v[here, h : h + 1] = logs[h * BLK : (h + 1) * BLK]

    half = 1024
    quarter = 256

    def project(it, lo, hi):
        for n in range(2048 // quarter):
            part = jnp.dot(
                heads[lo:hi, :], wo_v[:, n * quarter : (n + 1) * quarter], preferred_element_type=jnp.float32
            )
            c = n * quarter % half
            stage[it, n * quarter // half, lo:hi, c : c + quarter] = part.astype(jnp.bfloat16)

    def first(h):
        return remote(stage.at[0, h], got.at[h], snd_sem.at[h], got_sem.at[h], me, right if h == 0 else left)

    def move(k):
        it, h, nb = ((1, 1, right), (2, 0, left), (1, 0, right), (2, 1, left))[k]
        return remote(stage.at[it, h], got.at[2 + k], snd_sem.at[2 + k], got_sem.at[2 + k], me, nb)

    scores(3 * dest(0), 0)

    @pl.loop(0, TP)
    def _(it):
        b0 = 3 * dest(it)
        nxt = jnp.where(it == TP - 1, b0, 3 * dest(it + 1))
        for j in range(3):
            scores(b0 + j + 1 if j < 2 else nxt, (j + 1) % 3)
            values(b0 + j, j, j)
        project(it, 0, 3 * BLK)

        @pl.when(it == 0)
        def _():
            first(0).start()
            first(1).start()

        @pl.when(it == 1)
        def _():
            move(0).start()

        @pl.when(it == 2)
        def _():
            move(1).start()

    f32 = jnp.float32
    for h in range(2):
        first(h).wait_recv()
        stage[1 + h, h] = (stage[1 + h, h].astype(f32) + got[h].astype(f32)).astype(jnp.bfloat16)
        move(2 + h).start()
    log_ref[...] = jnp.transpose(log_v[...])[0:HEADS]
    for h in range(2):
        move(1 - h).wait_recv()
        move(2 + h).wait_recv()
        total = stage[3, h].astype(f32) + got[3 - h].astype(f32) + got[4 + h].astype(f32)
        out_ref[:, h * half : (h + 1) * half] = total.astype(jnp.bfloat16)
    for h in range(2):
        first(h).wait_send()
    for k in range(4):
        move(k).wait_send()

    for dist in dists:
        z = mz - dist

        @pl.when(have(dist))
        def _(z=z):
            to_right(z).wait_send()
            to_left(z).wait_send()
            pass_right(z).wait_send()

    for delta in order[:1] + order[-4:]:
        each(delta, lambda d: data_copy(d).wait_send())

    @pl.loop(0, me)
    def _(i):
        req_copy(i).wait_send()


def local(tokens, w_query, w_latent, latent_gain, w_output, chosen):
    vmem = pl.BlockSpec(memory_space=pltpu.VMEM)
    hbm = pl.BlockSpec(memory_space=pltpu.HBM)
    dma = pltpu.SemaphoreType.DMA
    bf16 = jnp.bfloat16
    part = ROWS // TP
    attended, logs = pl.pallas_call(
        kernel,
        out_shape=(
            jax.ShapeDtypeStruct((part, 2048), bf16),
            jax.ShapeDtypeStruct((HEADS, ROWS), jnp.float32),
        ),
        in_specs=[hbm, hbm, hbm, vmem, hbm, vmem],
        out_specs=(vmem, vmem),
        scratch_shapes=[
            pltpu.VMEM(tokens.shape, bf16),
            pltpu.VMEM(w_query.shape, bf16),
            pltpu.VMEM(w_latent.shape, bf16),
            pltpu.VMEM(w_output.shape, bf16),
            pltpu.VMEM((2 * PER, HALF, R), bf16),
            pltpu.VMEM((KV, HALF, R), bf16),
            pltpu.VMEM((SLOTS, HALF, R), bf16),
            pltpu.VMEM((ROWS, HEADS * R), bf16),
            pltpu.VMEM((KV, 1, 128), jnp.int32),
            pltpu.VMEM((KV, 1, 128), jnp.int32),
            pltpu.VMEM((3, 16, 128), jnp.int32),
            pltpu.SMEM((KV, 1, 128), jnp.int32),
            pltpu.SMEM((3, 16, 128), jnp.int32),
            pltpu.VMEM((3, NSEL * BLK, R), bf16),
            pltpu.VMEM((3, HEADS * BLK, NSEL * BLK), jnp.float32),
            pltpu.VMEM((3, HEADS * BLK, 128), jnp.float32),
            pltpu.VMEM((part, HEADS * R), bf16),
            pltpu.VMEM((TP, 2, part, 1024), bf16),
            pltpu.VMEM((6, part, 1024), bf16),
            pltpu.VMEM((ROWS, 128), jnp.float32),
            dma((6,)),
            dma((HEADS,)),
            dma,
            dma,
            dma,
            dma((KV,)),
            dma((KV,)),
            dma((KV,)),
            dma((2 * GRP,)),
            dma((3, GRP)),
            dma((GRP,)),
            dma((GRP,)),
            dma((GRP,)),
            dma((6,)),
            dma((6,)),
        ],
        compiler_params=pltpu.CompilerParams(
            collective_id=0, has_side_effects=True, vmem_limit_bytes=53 * 1024 * 1024
        ),
        name="layer",
    )(tokens, w_query, w_latent, latent_gain.reshape(1, R), w_output, chosen)
    return attended, logs.T


def solution(mesh):
    placed = (P("kv", None), P(None, "tp"), P(), P(), P("tp", None), P("kv", None))
    return jax.shard_map(
        local,
        mesh=mesh,
        in_specs=placed,
        out_specs=(P(("kv", "tp"), None), P("kv", "tp")),
        check_vma=False,
    )
```

```python
import functools

import jax
import jax.numpy as jnp
from jax import lax
from jax.experimental import pallas as pl
from jax.experimental.pallas import tpu as pltpu
from jax.sharding import PartitionSpec as P

EPS = 1e-06
KV = 64
TP = 4
GRP = 8
BLK = 64
HALF = 32
R = 256
PER = 12
NSEL = 32
OWN = TP * KV
SLOTS = OWN + 2 * PER
ROWS = PER * BLK
HEADS = 4


def remote(src, dst, send_sem, recv_sem, kv, tp):
    return pltpu.make_async_remote_copy(
        src_ref=src,
        dst_ref=dst,
        send_sem=send_sem,
        recv_sem=recv_sem,
        device_id={"kv": kv, "tp": tp},
        device_id_type=pl.DeviceIdType.MESH,
    )


def kernel(
    tok_hbm, wq_hbm, wl_hbm, gain_ref, wo_hbm, chosen_ref,
    out_ref, log_ref,
    tok_v, wq_v, wl_v, wo_v, own_v, sendbuf, table_ref, q_ref,
    req_v, idx_v, reqin, idx_ref,
    kbuf, s_scr, m_scr, heads, stage, got, log_v,
    tok_sem, wq_sem, wl_sem, wo_sem, loc_sem, rs_sem, rr_sem, ds_sem, dr_sem,
    xs_sem, xl_sem, xr_sem, xd_sem, snd_sem, got_sem,
):
    me = lax.axis_index("kv")
    x = lax.axis_index("tp")
    mz = me // GRP
    myc = me % GRP
    left = (x + TP - 1) % TP
    right = (x + 1) % TP
    barrier = pltpu.get_barrier_semaphore()

    @pl.loop(0, KV)
    def _(i):
        @pl.when(i != me)
        def _():
            pl.semaphore_signal(
                barrier, inc=1, device_id={"kv": i, "tp": x}, device_id_type=pl.DeviceIdType.MESH
            )

    for nb in (left, right):
        pl.semaphore_signal(
            barrier, inc=1, device_id={"kv": me, "tp": nb}, device_id_type=pl.DeviceIdType.MESH
        )

    def tok_copy(i):
        rows = pl.ds(i * 128, 128)
        return pltpu.make_async_copy(tok_hbm.at[rows], tok_v.at[rows], tok_sem.at[i])

    def wq_copy(h):
        cols = pl.ds(h * R, R)
        return pltpu.make_async_copy(wq_hbm.at[:, cols], wq_v.at[:, cols], wq_sem.at[h])

    wl_copy = pltpu.make_async_copy(wl_hbm, wl_v, wl_sem)
    wo_copy = pltpu.make_async_copy(wo_hbm, wo_v, wo_sem)
    wl_copy.start()
    for i in range(6):
        tok_copy(i).start()

    def hits(shape, g):
        c = jnp.broadcast_to(chosen_ref[g : g + 1, :].reshape((1,) * (len(shape) - 1) + (NSEL,)), shape)
        return c, ((c * 683) >> 13) == lax.broadcasted_iota(jnp.int32, shape, 0)

    far = jnp.full((KV, 1, NSEL), KV * PER, jnp.int32)
    near = jnp.full((KV, 1, NSEL), -1, jnp.int32)
    for g in range(PER):
        c, hit = hits((KV, 1, NSEL), g)
        far = jnp.minimum(far, jnp.where(hit, c, KV * PER))
        near = jnp.maximum(near, jnp.where(hit, c, -1))
    lo = jnp.min(far, axis=2, keepdims=True)
    hi = jnp.max(near, axis=2, keepdims=True)
    own0 = lax.broadcasted_iota(jnp.int32, (KV, 1, 1), 0) * PER
    pick = jnp.clip(jnp.where(x < 2, lo, hi) - own0, 0, PER - 1) * 2 + x % 2
    req_v[...] = jnp.broadcast_to(pick, req_v.shape)

    pl.semaphore_wait(barrier, KV - 1 + 2)

    def req_copy(i):
        return remote(req_v.at[i], reqin.at[me], rs_sem.at[i], rr_sem.at[me], i, x)

    @pl.loop(0, me)
    def _(i):
        req_copy(i).start()

    wl_copy.wait()
    for i in range(6):
        tok_copy(i).wait()
        p = jnp.dot(tok_v[i * 128 : (i + 1) * 128, :], wl_v[...], preferred_element_type=jnp.float32)
        inv = lax.rsqrt(jnp.mean(p * p, axis=-1, keepdims=True) + EPS)
        lat = (p * inv * gain_ref[...]).astype(jnp.bfloat16)
        own_v[4 * i : 4 * i + 4] = lat.reshape(4, HALF, R)
        table_ref[OWN + 4 * i : OWN + 4 * i + 4] = lat.reshape(4, HALF, R)

    for h in range(HEADS):
        wq_copy(h).start()
    wo_copy.start()

    def data_copy(d):
        return remote(
            sendbuf.at[d],
            table_ref.at[x * KV + me],
            ds_sem.at[d],
            dr_sem.at[jnp.where(d // GRP == mz, GRP + myc, mz)],
            d,
            x,
        )

    def each(delta, action):
        @pl.when(mz + delta < GRP)
        def _():
            @pl.loop(0, GRP)
            def _(k):
                d = (mz + delta) * GRP + (myc + k) % GRP

                @pl.when(d > me)
                def _():
                    action(d)

    def asked(d):
        remote(req_v.at[d], reqin.at[d], rs_sem.at[d], rr_sem.at[d], d, x).wait_recv()

    def fill(d):
        sendbuf[d] = own_v[reqin[d, 0, 0]]

    order = (0, 1, 7, 2, 6, 3, 5, 4)

    def send_group(s):
        each(order[s], asked)
        each(order[s], fill)
        if s >= 5:
            each(order[s - 4], lambda d: data_copy(d).wait_send())
        each(order[s], lambda d: data_copy(d).start())

    def project_query(h):
        wq_copy(h).wait()
        q = jnp.dot(tok_v[...], wq_v[:, h * R : (h + 1) * R], preferred_element_type=jnp.float32)
        q_ref[:, h * R : (h + 1) * R] = (q.astype(jnp.bfloat16).astype(jnp.float32) * (R ** -0.5)).astype(jnp.bfloat16)

    def region(quarter, z):
        return table_ref.at[pl.ds(quarter * KV + z * GRP, GRP)]

    def to_right(z):
        return remote(region(x, z), region(x, z), xs_sem.at[0, z], xl_sem.at[z], me, right)

    def to_left(z):
        return remote(region(x, z), region(x, z), xs_sem.at[1, z], xr_sem.at[z], me, left)

    def pass_right(z):
        return remote(region(left, z), region(left, z), xs_sem.at[2, z], xd_sem.at[z], me, right)

    def pass_left(z):
        return remote(region(right, z), region(right, z), xs_sem.at[2, z], xd_sem.at[z], me, left)

    for s in range(5):
        send_group(s)
    project_query(0)
    project_query(1)

    @pl.when(myc > 0)
    def _():
        @pl.loop(0, myc)
        def _(k):
            one = table_ref.at[x * KV + mz * GRP + k]
            pltpu.make_async_copy(one, one, dr_sem.at[GRP + k]).wait()

        to_right(mz).start()
        to_left(mz).start()

    send_group(5)
    project_query(2)
    send_group(6)
    project_query(3)
    send_group(7)
    far = jnp.full((KV, NSEL), KV * PER, jnp.int32)
    for g in range(PER):
        c, hit = hits((KV, NSEL), g)
        far = jnp.minimum(far, jnp.where(hit, c, KV * PER))
    lo = jnp.min(far, axis=1, keepdims=True)
    for g in range(PER):
        c, hit = hits((KV, NSEL), g)
        later = jnp.max(jnp.where(hit & (c > lo), 1, 0), axis=0, keepdims=True)
        c = chosen_ref[g : g + 1, :]
        owner = (c * 683) >> 13
        mine = owner == me
        valid = c >= 0
        first = jnp.where(mine, OWN + 2 * (c - me * PER), 2 * KV * later + owner)
        second = first + jnp.where(mine, 1, KV)
        idx_v[0, g : g + 1, 0:NSEL] = jnp.where(valid, first, OWN)
        idx_v[1, g : g + 1, 0:NSEL] = jnp.where(valid, second, OWN)
        live = jnp.sum(jnp.where(valid, 1, 0), axis=1, keepdims=True)
        idx_v[2, g : g + 1, :] = jnp.broadcast_to(live, (1, 128))
    idx_copy = pltpu.make_async_copy(idx_v, idx_ref, loc_sem)
    idx_copy.start()

    dists = (0, 1, 7, 2, 6, 3, 5, 4)

    def have(dist):
        return (mz >= dist) if dist else (myc > 0)

    def share(dist, only=None):
        @pl.when((mz >= dist) if only is None else (mz == only))
        def _():
            z = mz - dist
            pltpu.make_async_copy(region(x, z), region(x, z), dr_sem.at[z]).wait()
            to_right(z).start()
            to_left(z).start()

    def relay(dist):
        @pl.when(have(dist))
        def _():
            z = mz - dist
            to_right(z).wait_recv()
            to_left(z).wait_recv()

            @pl.when(z % 2 == 0)
            def _():
                pass_right(z).start()

            @pl.when(z % 2 == 1)
            def _():
                pass_left(z).start()

    share(1)
    share(7)
    relay(0)
    share(2)
    relay(1)
    relay(7)
    share(6, GRP - 1)
    share(3)
    relay(2)
    share(6, 6)
    share(5)
    relay(6)
    share(4)
    relay(3)
    relay(5)
    relay(4)

    idx_copy.wait()
    wo_copy.wait()
    for dist in dists:
        z = mz - dist

        @pl.when(have(dist))
        def _(z=z):
            pass_right(z).wait_recv()

    def dest(it):
        off = jnp.where(it == 0, 2, jnp.where(it == 1, 1, jnp.where(it == 2, 3, 0)))
        return (x + off) % TP

    rows = HEADS * BLK
    keys = NSEL * BLK
    step = 512

    def scores(b, slot):
        for j in range(2 * NSEL):
            kbuf[slot, j * HALF : (j + 1) * HALF, :] = table_ref[idx_ref[j % 2, b, j // 2]]
        here = pl.ds(pl.multiple_of(b * BLK, BLK), BLK)
        q = jnp.concatenate([q_ref[here, h * R : (h + 1) * R] for h in range(HEADS)], axis=0)
        live = idx_ref[2, b, 0] * BLK
        top = None
        for c in range(keys // step):
            s = lax.dot_general(
                q, kbuf[slot, c * step : (c + 1) * step, :], (((1,), (1,)), ((), ())),
                preferred_element_type=jnp.float32,
            )
            col = lax.broadcasted_iota(jnp.int32, (rows, step), 1)
            ok = col + c * step < live
            if c == 0:
                t = lax.broadcasted_iota(jnp.int32, (rows, step), 0) % BLK
                ok = ok & ((col >= BLK) | (col <= t))
            s = jnp.where(ok, s, -jnp.inf)
            s_scr[slot, :, c * step : (c + 1) * step] = s
            for k in range(step // 128):
                part = s[:, k * 128 : (k + 1) * 128]
                top = part if top is None else jnp.maximum(top, part)
        m_scr[slot] = top

    def values(b, slot, j):
        peak = jnp.max(m_scr[slot], axis=1, keepdims=True)
        total = None
        o = None
        for c in range(keys // step):
            e = jnp.exp(s_scr[slot, :, c * step : (c + 1) * step] - peak)
            for k in range(step // 128):
                part = e[:, k * 128 : (k + 1) * 128]
                total = part if total is None else total + part
            oc = jnp.dot(
                e.astype(jnp.bfloat16), kbuf[slot, c * step : (c + 1) * step, :],
                preferred_element_type=jnp.float32,
            )
            o = oc if o is None else o + oc
        mass = jnp.sum(total, axis=1, keepdims=True)
        o = o / mass
        logs = peak + jnp.log(mass)
        here = pl.ds(pl.multiple_of(b * BLK, BLK), BLK)
        for h in range(HEADS):
            heads[j * BLK : (j + 1) * BLK, h * R : (h + 1) * R] = o[h * BLK : (h + 1) * BLK].astype(jnp.bfloat16)
            log_v[here, h : h + 1] = logs[h * BLK : (h + 1) * BLK]

    half = 1024
    quarter = 256

    def project(it, lo, hi):
        for n in range(2048 // quarter):
            part = jnp.dot(
                heads[lo:hi, :], wo_v[:, n * quarter : (n + 1) * quarter], preferred_element_type=jnp.float32
            )
            c = n * quarter % half
            stage[it, n * quarter // half, lo:hi, c : c + quarter] = part.astype(jnp.bfloat16)

    def first(h):
        return remote(stage.at[0, h], got.at[h], snd_sem.at[h], got_sem.at[h], me, right if h == 0 else left)

    def move(k):
        it, h, nb = ((1, 1, right), (2, 0, left), (1, 0, right), (2, 1, left))[k]
        return remote(stage.at[it, h], got.at[2 + k], snd_sem.at[2 + k], got_sem.at[2 + k], me, nb)

    scores(3 * dest(0), 0)

    @pl.loop(0, TP)
    def _(it):
        b0 = 3 * dest(it)
        nxt = jnp.where(it == TP - 1, b0, 3 * dest(it + 1))
        for j in range(3):
            scores(b0 + j + 1 if j < 2 else nxt, (j + 1) % 3)
            values(b0 + j, j, j)
        project(it, 0, 3 * BLK)

        @pl.when(it == 0)
        def _():
            first(0).start()
            first(1).start()

        @pl.when(it == 1)
        def _():
            move(0).start()

        @pl.when(it == 2)
        def _():
            move(1).start()

    f32 = jnp.float32
    for h in range(2):
        first(h).wait_recv()
        stage[1 + h, h] = (stage[1 + h, h].astype(f32) + got[h].astype(f32)).astype(jnp.bfloat16)
        move(2 + h).start()
    log_ref[...] = jnp.transpose(log_v[...])[0:HEADS]
    for h in range(2):
        move(1 - h).wait_recv()
        move(2 + h).wait_recv()
        total = stage[3, h].astype(f32) + got[3 - h].astype(f32) + got[4 + h].astype(f32)
        out_ref[:, h * half : (h + 1) * half] = total.astype(jnp.bfloat16)
    for h in range(2):
        first(h).wait_send()
    for k in range(4):
        move(k).wait_send()

    for dist in dists:
        z = mz - dist

        @pl.when(have(dist))
        def _(z=z):
            to_right(z).wait_send()
            to_left(z).wait_send()
            pass_right(z).wait_send()

    for delta in order[:1] + order[-4:]:
        each(delta, lambda d: data_copy(d).wait_send())

    @pl.loop(0, me)
    def _(i):
        req_copy(i).wait_send()


def local(tokens, w_query, w_latent, latent_gain, w_output, chosen):
    vmem = pl.BlockSpec(memory_space=pltpu.VMEM)
    hbm = pl.BlockSpec(memory_space=pltpu.HBM)
    dma = pltpu.SemaphoreType.DMA
    bf16 = jnp.bfloat16
    part = ROWS // TP
    attended, logs = pl.pallas_call(
        kernel,
        out_shape=(
            jax.ShapeDtypeStruct((part, 2048), bf16),
            jax.ShapeDtypeStruct((HEADS, ROWS), jnp.float32),
        ),
        in_specs=[hbm, hbm, hbm, vmem, hbm, vmem],
        out_specs=(vmem, vmem),
        scratch_shapes=[
            pltpu.VMEM(tokens.shape, bf16),
            pltpu.VMEM(w_query.shape, bf16),
            pltpu.VMEM(w_latent.shape, bf16),
            pltpu.VMEM(w_output.shape, bf16),
            pltpu.VMEM((2 * PER, HALF, R), bf16),
            pltpu.VMEM((KV, HALF, R), bf16),
            pltpu.VMEM((SLOTS, HALF, R), bf16),
            pltpu.VMEM((ROWS, HEADS * R), bf16),
            pltpu.VMEM((KV, 1, 128), jnp.int32),
            pltpu.VMEM((3, 16, 128), jnp.int32),
            pltpu.SMEM((KV, 1, 128), jnp.int32),
            pltpu.SMEM((3, 16, 128), jnp.int32),
            pltpu.VMEM((3, NSEL * BLK, R), bf16),
            pltpu.VMEM((3, HEADS * BLK, NSEL * BLK), jnp.float32),
            pltpu.VMEM((3, HEADS * BLK, 128), jnp.float32),
            pltpu.VMEM((part, HEADS * R), bf16),
            pltpu.VMEM((TP, 2, part, 1024), bf16),
            pltpu.VMEM((6, part, 1024), bf16),
            pltpu.VMEM((ROWS, 128), jnp.float32),
            dma((6,)),
            dma((HEADS,)),
            dma,
            dma,
            dma,
            dma((KV,)),
            dma((KV,)),
            dma((KV,)),
            dma((2 * GRP,)),
            dma((3, GRP)),
            dma((GRP,)),
            dma((GRP,)),
            dma((GRP,)),
            dma((6,)),
            dma((6,)),
        ],
        compiler_params=pltpu.CompilerParams(
            collective_id=0, has_side_effects=True, vmem_limit_bytes=53 * 1024 * 1024
        ),
        name="layer",
    )(tokens, w_query, w_latent, latent_gain.reshape(1, R), w_output, chosen)
    return attended, logs.T


def solution(mesh):
    placed = (P("kv", None), P(None, "tp"), P(), P(), P("tp", None), P("kv", None))
    return jax.shard_map(
        local,
        mesh=mesh,
        in_specs=placed,
        out_specs=(P(("kv", "tp"), None), P("kv", "tp")),
        check_vma=False,
    )
```

```python
import functools

import jax
import jax.numpy as jnp
from jax import lax
from jax.experimental import pallas as pl
from jax.experimental.pallas import tpu as pltpu
from jax.sharding import PartitionSpec as P

EPS = 1e-06
KV = 64
TP = 4
GRP = 8
BLK = 64
HALF = 32
R = 256
PER = 12
NSEL = 32
OWN = TP * KV
SLOTS = OWN + 2 * PER
ROWS = PER * BLK
HEADS = 4


def remote(src, dst, send_sem, recv_sem, kv, tp):
    return pltpu.make_async_remote_copy(
        src_ref=src,
        dst_ref=dst,
        send_sem=send_sem,
        recv_sem=recv_sem,
        device_id={"kv": kv, "tp": tp},
        device_id_type=pl.DeviceIdType.MESH,
    )


def kernel(
    tok_hbm, wq_hbm, wl_hbm, gain_ref, wo_hbm, chosen_ref,
    out_ref, log_ref,
    tok_v, wq_v, wl_v, wo_v, own_v, sendbuf, table_ref, q_ref,
    req_v, idx_v, reqin, idx_ref,
    kbuf, s_scr, m_scr, heads, stage, got, log_v,
    tok_sem, wq_sem, wl_sem, wo_sem, loc_sem, rs_sem, rr_sem, ds_sem, dr_sem,
    xs_sem, xl_sem, xr_sem, xd_sem, snd_sem, got_sem,
):
    me = lax.axis_index("kv")
    x = lax.axis_index("tp")
    mz = me // GRP
    myc = me % GRP
    left = (x + TP - 1) % TP
    right = (x + 1) % TP
    barrier = pltpu.get_barrier_semaphore()

    @pl.loop(0, KV)
    def _(i):
        @pl.when(i != me)
        def _():
            pl.semaphore_signal(
                barrier, inc=1, device_id={"kv": i, "tp": x}, device_id_type=pl.DeviceIdType.MESH
            )

    for nb in (left, right):
        pl.semaphore_signal(
            barrier, inc=1, device_id={"kv": me, "tp": nb}, device_id_type=pl.DeviceIdType.MESH
        )

    def tok_copy(i):
        rows = pl.ds(i * 128, 128)
        return pltpu.make_async_copy(tok_hbm.at[rows], tok_v.at[rows], tok_sem.at[i])

    def wq_copy(h):
        cols = pl.ds(h * R, R)
        return pltpu.make_async_copy(wq_hbm.at[:, cols], wq_v.at[:, cols], wq_sem.at[h])

    wl_copy = pltpu.make_async_copy(wl_hbm, wl_v, wl_sem)
    wo_copy = pltpu.make_async_copy(wo_hbm, wo_v, wo_sem)
    wl_copy.start()
    for i in range(6):
        tok_copy(i).start()

    def hits(shape, g):
        c = jnp.broadcast_to(chosen_ref[g : g + 1, :].reshape((1,) * (len(shape) - 1) + (NSEL,)), shape)
        return c, ((c * 683) >> 13) == lax.broadcasted_iota(jnp.int32, shape, 0)

    far = jnp.full((KV, 1, NSEL), KV * PER, jnp.int32)
    near = jnp.full((KV, 1, NSEL), -1, jnp.int32)
    for g in range(PER):
        c, hit = hits((KV, 1, NSEL), g)
        far = jnp.minimum(far, jnp.where(hit, c, KV * PER))
        near = jnp.maximum(near, jnp.where(hit, c, -1))
    lo = jnp.min(far, axis=2, keepdims=True)
    hi = jnp.max(near, axis=2, keepdims=True)
    own0 = lax.broadcasted_iota(jnp.int32, (KV, 1, 1), 0) * PER
    pick = jnp.clip(jnp.where(x < 2, lo, hi) - own0, 0, PER - 1) * 2 + x % 2
    req_v[...] = jnp.broadcast_to(pick, req_v.shape)

    pl.semaphore_wait(barrier, KV - 1 + 2)

    def req_copy(i):
        return remote(req_v.at[i], reqin.at[me], rs_sem.at[i], rr_sem.at[me], i, x)

    @pl.loop(0, me)
    def _(i):
        req_copy(i).start()

    wl_copy.wait()
    for i in range(6):
        tok_copy(i).wait()
        p = jnp.dot(tok_v[i * 128 : (i + 1) * 128, :], wl_v[...], preferred_element_type=jnp.float32)
        inv = lax.rsqrt(jnp.mean(p * p, axis=-1, keepdims=True) + EPS)
        lat = (p * inv * gain_ref[...]).astype(jnp.bfloat16)
        own_v[4 * i : 4 * i + 4] = lat.reshape(4, HALF, R)
        table_ref[OWN + 4 * i : OWN + 4 * i + 4] = lat.reshape(4, HALF, R)

    for h in range(HEADS):
        wq_copy(h).start()
    wo_copy.start()

    def data_copy(d):
        return remote(
            sendbuf.at[d],
            table_ref.at[x * KV + me],
            ds_sem.at[d],
            dr_sem.at[jnp.where(d // GRP == mz, GRP + myc, mz)],
            d,
            x,
        )

    def each(delta, action):
        @pl.when(mz + delta < GRP)
        def _():
            @pl.loop(0, GRP)
            def _(k):
                d = (mz + delta) * GRP + (myc + k) % GRP

                @pl.when(d > me)
                def _():
                    action(d)

    def asked(d):
        remote(req_v.at[d], reqin.at[d], rs_sem.at[d], rr_sem.at[d], d, x).wait_recv()

    def fill(d):
        sendbuf[d] = own_v[reqin[d, 0, 0]]

    order = (0, 1, 7, 2, 6, 3, 5, 4)

    def send_group(s):
        each(order[s], asked)
        each(order[s], fill)
        each(order[s], lambda d: data_copy(d).start())

    def project_query(h):
        wq_copy(h).wait()
        q = jnp.dot(tok_v[...], wq_v[:, h * R : (h + 1) * R], preferred_element_type=jnp.float32)
        q_ref[:, h * R : (h + 1) * R] = (q.astype(jnp.bfloat16).astype(jnp.float32) * (R ** -0.5)).astype(jnp.bfloat16)

    def region(quarter, z):
        return table_ref.at[pl.ds(quarter * KV + z * GRP, GRP)]

    def to_right(z):
        return remote(region(x, z), region(x, z), xs_sem.at[0, z], xl_sem.at[z], me, right)

    def to_left(z):
        return remote(region(x, z), region(x, z), xs_sem.at[1, z], xr_sem.at[z], me, left)

    def pass_right(z):
        return remote(region(left, z), region(left, z), xs_sem.at[2, z], xd_sem.at[z], me, right)

    def pass_left(z):
        return remote(region(right, z), region(right, z), xs_sem.at[2, z], xd_sem.at[z], me, left)

    for s in range(5):
        send_group(s)
    project_query(0)
    project_query(1)

    @pl.when(myc > 0)
    def _():
        @pl.loop(0, myc)
        def _(k):
            one = table_ref.at[x * KV + mz * GRP + k]
            pltpu.make_async_copy(one, one, dr_sem.at[GRP + k]).wait()

        to_right(mz).start()
        to_left(mz).start()

    send_group(5)
    project_query(2)
    send_group(6)
    project_query(3)
    send_group(7)
    far = jnp.full((KV, NSEL), KV * PER, jnp.int32)
    for g in range(PER):
        c, hit = hits((KV, NSEL), g)
        far = jnp.minimum(far, jnp.where(hit, c, KV * PER))
    lo = jnp.min(far, axis=1, keepdims=True)
    for g in range(PER):
        c, hit = hits((KV, NSEL), g)
        later = jnp.max(jnp.where(hit & (c > lo), 1, 0), axis=0, keepdims=True)
        c = chosen_ref[g : g + 1, :]
        owner = (c * 683) >> 13
        mine = owner == me
        valid = c >= 0
        first = jnp.where(mine, OWN + 2 * (c - me * PER), 2 * KV * later + owner)
        second = first + jnp.where(mine, 1, KV)
        idx_v[0, g : g + 1, 0:NSEL] = jnp.where(valid, first, OWN)
        idx_v[1, g : g + 1, 0:NSEL] = jnp.where(valid, second, OWN)
        live = jnp.sum(jnp.where(valid, 1, 0), axis=1, keepdims=True)
        idx_v[2, g : g + 1, :] = jnp.broadcast_to(live, (1, 128))
    idx_copy = pltpu.make_async_copy(idx_v, idx_ref, loc_sem)
    idx_copy.start()

    dists = (0, 1, 7, 2, 6, 3, 5, 4)

    def have(dist):
        return (mz >= dist) if dist else (myc > 0)

    def share(dist, only=None):
        @pl.when((mz >= dist) if only is None else (mz == only))
        def _():
            z = mz - dist
            pltpu.make_async_copy(region(x, z), region(x, z), dr_sem.at[z]).wait()
            to_right(z).start()
            to_left(z).start()

    def relay(dist):
        @pl.when(have(dist))
        def _():
            z = mz - dist
            to_right(z).wait_recv()
            to_left(z).wait_recv()

            @pl.when(z % 2 == 0)
            def _():
                pass_right(z).start()

            @pl.when(z % 2 == 1)
            def _():
                pass_left(z).start()

    share(1)
    share(7)
    relay(0)
    share(2)
    relay(1)
    relay(7)
    share(6, GRP - 1)
    share(3)
    relay(2)
    share(6, 6)
    share(5)
    relay(6)
    share(4)
    relay(3)
    relay(5)
    relay(4)

    idx_copy.wait()
    wo_copy.wait()
    for dist in dists:
        z = mz - dist

        @pl.when(have(dist))
        def _(z=z):
            pass_right(z).wait_recv()

    def dest(it):
        off = jnp.where(it == 0, 2, jnp.where(it == 1, 1, jnp.where(it == 2, 3, 0)))
        return (x + off) % TP

    rows = HEADS * BLK
    keys = NSEL * BLK
    step = 512

    def scores(b, slot):
        for j in range(2 * NSEL):
            kbuf[slot, j * HALF : (j + 1) * HALF, :] = table_ref[idx_ref[j % 2, b, j // 2]]
        here = pl.ds(pl.multiple_of(b * BLK, BLK), BLK)
        q = jnp.concatenate([q_ref[here, h * R : (h + 1) * R] for h in range(HEADS)], axis=0)
        live = idx_ref[2, b, 0] * BLK
        top = None
        for c in range(keys // step):
            s = lax.dot_general(
                q, kbuf[slot, c * step : (c + 1) * step, :], (((1,), (1,)), ((), ())),
                preferred_element_type=jnp.float32,
            )
            col = lax.broadcasted_iota(jnp.int32, (rows, step), 1)
            ok = col + c * step < live
            if c == 0:
                t = lax.broadcasted_iota(jnp.int32, (rows, step), 0) % BLK
                ok = ok & ((col >= BLK) | (col <= t))
            s = jnp.where(ok, s, -jnp.inf)
            s_scr[slot, :, c * step : (c + 1) * step] = s
            for k in range(step // 128):
                part = s[:, k * 128 : (k + 1) * 128]
                top = part if top is None else jnp.maximum(top, part)
        m_scr[slot] = top

    def values(b, slot, j):
        peak = jnp.max(m_scr[slot], axis=1, keepdims=True)
        total = None
        o = None
        for c in range(keys // step):
            e = jnp.exp(s_scr[slot, :, c * step : (c + 1) * step] - peak)
            for k in range(step // 128):
                part = e[:, k * 128 : (k + 1) * 128]
                total = part if total is None else total + part
            oc = jnp.dot(
                e.astype(jnp.bfloat16), kbuf[slot, c * step : (c + 1) * step, :],
                preferred_element_type=jnp.float32,
            )
            o = oc if o is None else o + oc
        mass = jnp.sum(total, axis=1, keepdims=True)
        o = o / mass
        logs = peak + jnp.log(mass)
        here = pl.ds(pl.multiple_of(b * BLK, BLK), BLK)
        for h in range(HEADS):
            heads[j * BLK : (j + 1) * BLK, h * R : (h + 1) * R] = o[h * BLK : (h + 1) * BLK].astype(jnp.bfloat16)
            log_v[here, h : h + 1] = logs[h * BLK : (h + 1) * BLK]

    half = 1024
    quarter = 256

    def project(it, lo, hi):
        for n in range(2048 // quarter):
            part = jnp.dot(
                heads[lo:hi, :], wo_v[:, n * quarter : (n + 1) * quarter], preferred_element_type=jnp.float32
            )
            c = n * quarter % half
            stage[it, n * quarter // half, lo:hi, c : c + quarter] = part.astype(jnp.bfloat16)

    def first(h):
        return remote(stage.at[0, h], got.at[h], snd_sem.at[h], got_sem.at[h], me, right if h == 0 else left)

    def move(k):
        it, h, nb = ((1, 1, right), (2, 0, left), (1, 0, right), (2, 1, left))[k]
        return remote(stage.at[it, h], got.at[2 + k], snd_sem.at[2 + k], got_sem.at[2 + k], me, nb)

    scores(3 * dest(0), 0)

    @pl.loop(0, TP)
    def _(it):
        b0 = 3 * dest(it)
        nxt = jnp.where(it == TP - 1, b0, 3 * dest(it + 1))
        for j in range(3):
            scores(b0 + j + 1 if j < 2 else nxt, (j + 1) % 3)
            values(b0 + j, j, j)
        project(it, 0, 3 * BLK)

        @pl.when(it == 0)
        def _():
            first(0).start()
            first(1).start()

        @pl.when(it == 1)
        def _():
            move(0).start()

        @pl.when(it == 2)
        def _():
            move(1).start()

    f32 = jnp.float32
    for h in range(2):
        first(h).wait_recv()
        stage[1 + h, h] = (stage[1 + h, h].astype(f32) + got[h].astype(f32)).astype(jnp.bfloat16)
        move(2 + h).start()
    log_ref[...] = jnp.transpose(log_v[...])[0:HEADS]
    for h in range(2):
        move(1 - h).wait_recv()
        move(2 + h).wait_recv()
        total = stage[3, h].astype(f32) + got[3 - h].astype(f32) + got[4 + h].astype(f32)
        out_ref[:, h * half : (h + 1) * half] = total.astype(jnp.bfloat16)
    for h in range(2):
        first(h).wait_send()
    for k in range(4):
        move(k).wait_send()

    for dist in dists:
        z = mz - dist

        @pl.when(have(dist))
        def _(z=z):
            to_right(z).wait_send()
            to_left(z).wait_send()
            pass_right(z).wait_send()

    for delta in order:
        each(delta, lambda d: data_copy(d).wait_send())

    @pl.loop(0, me)
    def _(i):
        req_copy(i).wait_send()


def local(tokens, w_query, w_latent, latent_gain, w_output, chosen):
    vmem = pl.BlockSpec(memory_space=pltpu.VMEM)
    hbm = pl.BlockSpec(memory_space=pltpu.HBM)
    dma = pltpu.SemaphoreType.DMA
    bf16 = jnp.bfloat16
    part = ROWS // TP
    attended, logs = pl.pallas_call(
        kernel,
        out_shape=(
            jax.ShapeDtypeStruct((part, 2048), bf16),
            jax.ShapeDtypeStruct((HEADS, ROWS), jnp.float32),
        ),
        in_specs=[hbm, hbm, hbm, vmem, hbm, vmem],
        out_specs=(vmem, vmem),
        scratch_shapes=[
            pltpu.VMEM(tokens.shape, bf16),
            pltpu.VMEM(w_query.shape, bf16),
            pltpu.VMEM(w_latent.shape, bf16),
            pltpu.VMEM(w_output.shape, bf16),
            pltpu.VMEM((2 * PER, HALF, R), bf16),
            pltpu.VMEM((KV, HALF, R), bf16),
            pltpu.VMEM((SLOTS, HALF, R), bf16),
            pltpu.VMEM((ROWS, HEADS * R), bf16),
            pltpu.VMEM((KV, 1, 128), jnp.int32),
            pltpu.VMEM((3, 16, 128), jnp.int32),
            pltpu.SMEM((KV, 1, 128), jnp.int32),
            pltpu.SMEM((3, 16, 128), jnp.int32),
            pltpu.VMEM((3, NSEL * BLK, R), bf16),
            pltpu.VMEM((3, HEADS * BLK, NSEL * BLK), jnp.float32),
            pltpu.VMEM((3, HEADS * BLK, 128), jnp.float32),
            pltpu.VMEM((part, HEADS * R), bf16),
            pltpu.VMEM((TP, 2, part, 1024), bf16),
            pltpu.VMEM((6, part, 1024), bf16),
            pltpu.VMEM((ROWS, 128), jnp.float32),
            dma((6,)),
            dma((HEADS,)),
            dma,
            dma,
            dma,
            dma((KV,)),
            dma((KV,)),
            dma((KV,)),
            dma((2 * GRP,)),
            dma((3, GRP)),
            dma((GRP,)),
            dma((GRP,)),
            dma((GRP,)),
            dma((6,)),
            dma((6,)),
        ],
        compiler_params=pltpu.CompilerParams(
            collective_id=0, has_side_effects=True, vmem_limit_bytes=53 * 1024 * 1024
        ),
        name="layer",
    )(tokens, w_query, w_latent, latent_gain.reshape(1, R), w_output, chosen)
    return attended, logs.T


def solution(mesh):
    placed = (P("kv", None), P(None, "tp"), P(), P(), P("tp", None), P("kv", None))
    return jax.shard_map(
        local,
        mesh=mesh,
        in_specs=placed,
        out_specs=(P(("kv", "tp"), None), P("kv", "tp")),
        check_vma=False,
    )
```
